32 devices in a mesh: sp: 8 (over z, x), tp: 4 (over y, core).
Axes of the slice: x: 2, y: 2, z: 4, core: 2. Of those that a mesh axis runs over, the one named last changes fastest.
Arguments:
- queries: bfloat16 [1024, 2048], P('sp', 'tp'), may hold values from -6 to 6
- key_rows: bfloat16 [1024, 2048], P('sp', 'tp'), may hold values from -6 to 6
- value_rows: bfloat16 [1024, 2048], P('sp', 'tp'), may hold values from -6 to 6
- gate_input: bfloat16 [1024, 2048], P('sp', 'tp'), may hold values from -6 to 6
- log_decay: float32 [1024, 16], P('sp', 'tp'), may hold values from -0.6 to 0, as said below
- head_gain: float32 [2048], P('tp'), may hold values from 0.1 to 1.9
- out_weight: bfloat16 [2048, 2048], P('tp'), may hold values from -0.125 to 0.125
- residual: bfloat16 [1024, 2048], P('sp'), may hold values from -6 to 6
- mlp_gain: float32 [2048], replicated, may hold values from 0.1 to 1.9
- gate_weight: bfloat16 [2048, 5632], P('sp', 'tp'), may hold values from -0.125 to 0.125
- up_weight: bfloat16 [2048, 5632], P('sp', 'tp'), may hold values from -0.125 to 0.125
- down_weight: bfloat16 [5632, 2048], P('tp', 'sp'), may hold values from -0.078125 to 0.078125
Outputs:
- layer_out: bfloat16 [1024, 2048], P(('sp', 'tp'))
The draws below stay inside these ranges and needn't reach their ends.
Inputs may be any that keep to these rules, and one draw needn't show every extreme that they name: log_decay holds the logarithm of a decay factor of each head at each position.
All inputs are finite; a program needn't handle non-finite values.
Results may differ from the reference program's by a relative error of at most 0.017.
Values may be sent and summed in bfloat16 or wider, within the bound.
A program may use at most 128 MiB of HBM per device.

```python
import math
import jax
import jax.numpy as jnp
from jax import lax

D = 2048
RETENTION_HEADS = 16
HD = 128
FF = 5632
BLOCK = 128
TOK_DEV = 128
SEQUENCE_TOKENS = 1024
N_TP = 4


def draw_log_decay(key, part):
    key_collection = jax.random.split(jax.random.fold_in(key, 11), 5)
    slow_kind = jax.random.randint(key_collection[0], (RETENTION_HEADS,), 0, 10) < 5
    fast_length = jnp.exp(jax.random.uniform(key_collection[1], (RETENTION_HEADS,), jnp.float32, math.log(30.0), math.log(100.0)))
    fast_rate = -1.0 / fast_length
    device_blocks = SEQUENCE_TOKENS // TOK_DEV
    factor = jnp.exp(jax.random.uniform(key_collection[2], (device_blocks, RETENTION_HEADS), jnp.float32, math.log(0.4), math.log(1.6)))
    slow_rate = jnp.repeat(factor, TOK_DEV, axis=0) * (-0.4 / SEQUENCE_TOKENS)
    spike_positions = jax.random.randint(key_collection[3], (3, RETENTION_HEADS), 0, SEQUENCE_TOKENS)
    spike_length = jnp.log(jax.random.uniform(key_collection[4], (3, RETENTION_HEADS), jnp.float32, 0.6, 0.8))
    token_spots = jnp.arange(SEQUENCE_TOKENS, dtype=jnp.int32)[:, None, None]
    spike_rows = jnp.sum(jnp.where(token_spots == spike_positions[None], spike_length[None], 0.0), axis=1)
    constant_level = jnp.where(slow_kind[None, :], slow_rate, fast_rate[None, :])
    return (constant_level + spike_rows).astype(jnp.float32)


def levels(rng, shape, cuts, smallest, high):
    level = 1.0
    for dim, parts in cuts:
        heights = jax.random.uniform(jax.random.fold_in(jax.random.fold_in(rng, 6), dim), (parts,), jnp.float32, smallest / len(cuts), high / len(cuts))
        level = level * jnp.repeat(jnp.exp(heights), shape[dim] // parts).reshape((-1,) + (1,) * (len(shape) - 1 - dim))
    return level


def gaussian(own_key, shape, scale, reach, pieces=(), kind=jnp.bfloat16):
    drawn = scale * jax.random.normal(own_key, shape, jnp.float32)
    if pieces:
        drawn = drawn * levels(own_key, shape, pieces, -0.22, 0.18)
    return jnp.clip(drawn, -reach, reach).astype(kind)


def setup_inputs(seed: int = 0) -> dict:
    streams_of = jax.random.split(jax.random.key(seed), 13)
    return {
        "queries": gaussian(streams_of[0], (SEQUENCE_TOKENS, RETENTION_HEADS * HD), 1.0, 6.0, ((0, 8), (1, 4))),
        "key_rows": gaussian(streams_of[1], (SEQUENCE_TOKENS, RETENTION_HEADS * HD), 1.0, 6.0, ((0, 8), (1, 4))),
        "value_rows": gaussian(streams_of[2], (SEQUENCE_TOKENS, RETENTION_HEADS * HD), 1.0, 6.0, ((0, 8), (1, 4))),
        "gate_input": gaussian(streams_of[3], (SEQUENCE_TOKENS, RETENTION_HEADS * HD), 1.0, 6.0, ((0, 8), (1, 4))),
        "log_decay": draw_log_decay(jax.random.fold_in(streams_of[12], 71), 0),
        "head_gain": jnp.clip(1.0 + 0.18 * jax.random.normal(streams_of[5], (RETENTION_HEADS * HD,), jnp.float32), 0.1, 1.9),
        "out_weight": gaussian(streams_of[6], (RETENTION_HEADS * HD, D), (RETENTION_HEADS * HD) ** -0.5, 0.125, ((0, 4),)),
        "residual": gaussian(streams_of[7], (SEQUENCE_TOKENS, D), 1.0, 6.0, ((0, 8),)),
        "mlp_gain": jnp.clip(1.0 + 0.18 * jax.random.normal(streams_of[8], (D,), jnp.float32), 0.1, 1.9),
        "gate_weight": gaussian(streams_of[9], (D, FF), D ** -0.5, 0.125, ((0, 8), (1, 4))),
        "up_weight": gaussian(streams_of[10], (D, FF), D ** -0.5, 0.125, ((0, 8), (1, 4))),
        "down_weight": gaussian(streams_of[11], (FF, D), FF ** -0.5, 0.078125, ((0, 4), (1, 8))),
    }


EPS = 1e-06

def rotate(values_in, positions):
    half = values_in.shape[-1] // 2
    freq = 10000.0 ** (-jnp.linspace(0.0, 1.0, half, dtype=jnp.float32))
    angles = positions * freq
    angles = jnp.concatenate([angles, angles], axis=-1)
    first = values_in[..., :half]
    second = values_in[..., half:]
    turned = jnp.concatenate([-second, first], axis=-1)
    return values_in * jnp.cos(angles) + turned * jnp.sin(angles)

def row_norm(stream, gain):
    return stream * lax.rsqrt(lax.optimization_barrier(jnp.mean(stream * stream, axis=-1, keepdims=True)) + EPS) * gain

def retain_head(inputs):
    query_head, key_head, value_head, decay_head, gain_head = inputs
    length = query_head.shape[0]
    positions = jnp.arange(length, dtype=jnp.float32)[:, None]
    q_rot = rotate(query_head.astype(jnp.float32), positions).astype(jnp.bfloat16)
    k_rot = (rotate(key_head.astype(jnp.float32), positions) * HD ** (-0.5)).astype(jnp.bfloat16)
    blocks = length // BLOCK
    q_blocks = q_rot.reshape(blocks, BLOCK, HD).astype(jnp.float32)
    k_blocks = k_rot.reshape(blocks, BLOCK, HD).astype(jnp.float32)
    v_blocks = value_head.reshape(blocks, BLOCK, HD).astype(jnp.float32)
    cumul = jnp.cumsum(decay_head.reshape(blocks, BLOCK), axis=1)
    lower = jnp.tril(jnp.ones((BLOCK, BLOCK), dtype=bool))
    spread = cumul[:, :, None] - cumul[:, None, :]
    weight = jnp.where(lower, jnp.exp(jnp.where(lower, spread, 0.0)), 0.0)
    scores = jnp.einsum('ntd,nsd->nts', q_blocks, k_blocks)
    probs = (scores * weight).astype(jnp.bfloat16).astype(jnp.float32)
    inner = jnp.einsum('nts,nse->nte', probs, v_blocks)
    k_weighted = (k_blocks * jnp.exp(cumul[:, -1:] - cumul)[:, :, None]).astype(jnp.bfloat16).astype(jnp.float32)
    contrib = jnp.einsum('nsd,nse->nde', k_weighted, v_blocks)
    totals = jnp.exp(cumul[:, -1])

    def advance(state, items):
        factor, update = items
        return (state * factor + update, state)
    _, before = lax.scan(advance, jnp.zeros((HD, HD), jnp.float32), (totals, contrib))
    cross = jnp.einsum('ntd,nde->nte', q_blocks, before, precision=lax.Precision.HIGHEST)
    cross = cross * jnp.exp(cumul)[:, :, None]
    result = (inner + cross).reshape(length, HD)
    return row_norm(result, gain_head)

def reference(queries, key_rows, value_rows, gate_input, log_decay, head_gain, out_weight, residual, mlp_gain, gate_weight, up_weight, down_weight):

    def by_head(array):
        return array.reshape(SEQUENCE_TOKENS, RETENTION_HEADS, HD).transpose(1, 0, 2)
    heads_out = lax.map(retain_head, (by_head(queries), by_head(key_rows), by_head(value_rows), log_decay.T, head_gain.reshape(RETENTION_HEADS, HD)))
    joined = heads_out.transpose(1, 0, 2).reshape(SEQUENCE_TOKENS, RETENTION_HEADS * HD)
    gate_act = jax.nn.silu(gate_input.astype(jnp.float32))
    retained = (joined * gate_act).astype(jnp.bfloat16)
    width = RETENTION_HEADS * HD // N_TP
    hidden_width = FF // N_TP

    def layer_block(items):
        ret_rows, res_rows = items
        mixed = jnp.zeros((TOK_DEV, D), jnp.float32)
        for group_idx in range(N_TP):
            part = jnp.dot(ret_rows[:, group_idx * width:(group_idx + 1) * width], out_weight[group_idx * width:(group_idx + 1) * width], preferred_element_type=jnp.float32)
            part = lax.optimization_barrier(part.astype(jnp.bfloat16))
            mixed = mixed + part.astype(jnp.float32)
        middle = (res_rows.astype(jnp.float32) + mixed).astype(jnp.bfloat16)
        normed = row_norm(middle.astype(jnp.float32), mlp_gain).astype(jnp.bfloat16)
        gate = jnp.dot(normed, gate_weight, preferred_element_type=jnp.float32)
        upvals = jnp.dot(normed, up_weight, preferred_element_type=jnp.float32)
        hidden = (jax.nn.silu(gate) * upvals).astype(jnp.bfloat16)
        ffn = jnp.zeros((TOK_DEV, D), jnp.float32)
        for group_idx in range(N_TP):
            part = jnp.dot(hidden[:, group_idx * hidden_width:(group_idx + 1) * hidden_width], down_weight[group_idx * hidden_width:(group_idx + 1) * hidden_width], preferred_element_type=jnp.float32)
            part = lax.optimization_barrier(part.astype(jnp.bfloat16))
            ffn = ffn + part.astype(jnp.float32)
        return (middle.astype(jnp.float32) + ffn).astype(jnp.bfloat16)
    outcome = lax.map(layer_block, (retained.reshape(-1, TOK_DEV, RETENTION_HEADS * HD), residual.reshape(-1, TOK_DEV, D)))
    return outcome.reshape(SEQUENCE_TOKENS, D)
```

```python
import functools

import jax
import jax.numpy as jnp
from jax import lax
from jax.experimental import pallas as pl
from jax.experimental.pallas import tpu as pltpu
from jax.sharding import PartitionSpec as P

BLOCK = 128


EPS = 1e-06


def prefix_2(x, axis, join, neutral):
    place = lax.axis_index(axis)
    gathered = jax.tree.map(
        lambda a, kind: lax.all_gather(a.astype(kind), axis), x, (jnp.bfloat16, jnp.bfloat16)
    )
    state = jax.tree.map(lambda a, e: jnp.zeros_like(a) + jnp.asarray(e, a.dtype), x, neutral)

    def one(step, state):
        return join(
            state,
            jax.tree.map(
                lambda a, own: lax.dynamic_index_in_dim(a, step, 0, False).astype(own.dtype),
                gathered,
                x,
            ),
        )

    return lax.fori_loop(0, place, one, state)


def rotate(values_in, positions):
    half = values_in.shape[-1] // 2
    freq = 10000.0 ** (-jnp.linspace(0.0, 1.0, half, dtype=jnp.float32))
    angles = positions * freq
    angles = jnp.concatenate([angles, angles], axis=-1)
    first = values_in[..., :half]
    second = values_in[..., half:]
    turned = jnp.concatenate([-second, first], axis=-1)
    return values_in * jnp.cos(angles) + turned * jnp.sin(angles)


def row_norm(stream, gain):
    return stream * lax.rsqrt(jnp.mean(stream * stream, axis=-1, keepdims=True) + EPS) * gain


def join_states(earlier, later):
    return (earlier[0] * later[0], later[0][:, None, None] * earlier[1] + later[1])


def body(
    queries,
    key_rows,
    value_rows,
    gate_input,
    log_decay,
    head_gain,
    out_weight,
    residual,
    mlp_gain,
    gate_weight,
    up_weight,
    down_weight,
):
    tok_rows = queries.shape[0]
    heads_here = log_decay.shape[1]
    head_size = head_gain.shape[0] // heads_here
    quarter = tok_rows // lax.axis_size("tp")
    offset = lax.axis_index("sp") * tok_rows
    positions = (offset + lax.iota(jnp.int32, tok_rows)).astype(jnp.float32)[:, None, None]
    q_rot = rotate(
        queries.reshape(tok_rows, heads_here, head_size).astype(jnp.float32), positions
    ).astype(jnp.bfloat16)
    k_rot = (
        rotate(key_rows.reshape(tok_rows, heads_here, head_size).astype(jnp.float32), positions)
        * head_size ** (-0.5)
    ).astype(jnp.bfloat16)
    blocks = tok_rows // BLOCK
    q_blocks = q_rot.reshape(blocks, BLOCK, heads_here, head_size)
    k_blocks = k_rot.reshape(blocks, BLOCK, heads_here, head_size)
    v_blocks = value_rows.reshape(blocks, BLOCK, heads_here, head_size)
    cumul = jnp.cumsum(log_decay.reshape(blocks, BLOCK, heads_here), axis=1)
    by_head = cumul.transpose(0, 2, 1)
    lower = jnp.tril(jnp.ones((BLOCK, BLOCK), dtype=bool))
    spread = by_head[:, :, :, None] - by_head[:, :, None, :]
    weight = jnp.where(lower, jnp.exp(jnp.where(lower, spread, 0.0)), 0.0)
    scores = jnp.einsum("nthd,nshd->nhts", q_blocks, k_blocks, preferred_element_type=jnp.float32)
    probs = (scores * weight).astype(jnp.bfloat16)
    inner = jnp.einsum("nhts,nshe->nthe", probs, v_blocks, preferred_element_type=jnp.float32)
    k_weighted = (
        k_blocks.astype(jnp.float32) * jnp.exp(cumul[:, -1:, :] - cumul)[..., None]
    ).astype(jnp.bfloat16)
    contrib = jnp.einsum(
        "nshd,nshe->nhde", k_weighted, v_blocks, preferred_element_type=jnp.float32
    )
    totals = jnp.exp(cumul[:, -1, :])

    def advance(carry, items):
        state, prefix = carry
        factor, update = items
        return ((state * factor[:, None, None] + update, prefix * factor), (state, prefix))

    start_state = jnp.zeros((heads_here, head_size, head_size), jnp.float32)
    start_prefix = jnp.ones((heads_here,), jnp.float32)
    (dev_state, dev_total), (local_before, prefixes) = lax.scan(
        advance, (start_state, start_prefix), (totals, contrib)
    )
    _, incoming = prefix_2((dev_total, dev_state), "sp", join_states, (start_prefix, start_state))
    before = local_before + prefixes[:, :, None, None] * incoming[None]
    cross = jnp.einsum(
        "nthd,nhde->nthe", q_blocks.astype(jnp.float32), before, precision=lax.Precision.HIGHEST
    )
    cross = cross * jnp.exp(cumul)[..., None]
    result = (inner + cross).reshape(tok_rows, heads_here, head_size)
    result = row_norm(result, head_gain.reshape(heads_here, head_size)).reshape(
        tok_rows, heads_here * head_size
    )
    retained = (result * jax.nn.silu(gate_input.astype(jnp.float32))).astype(jnp.bfloat16)
    picked = retained
    mixed = lax.psum_scatter(
        jnp.dot(picked, out_weight, preferred_element_type=jnp.float32).astype(jnp.bfloat16),
        "tp",
        scatter_dimension=0,
        tiled=True,
    ).astype(jnp.float32)
    own_rows = lax.dynamic_slice_in_dim(residual, lax.axis_index("tp") * quarter, quarter, 0)
    rows_mid = (own_rows.astype(jnp.float32) + mixed).astype(jnp.bfloat16)
    own_normed = row_norm(rows_mid.astype(jnp.float32), mlp_gain).astype(jnp.bfloat16)
    normed = lax.all_gather(own_normed, "tp", axis=0, tiled=True)
    gate = jnp.dot(
        normed,
        lax.all_gather(gate_weight, "sp", axis=0, tiled=True),
        preferred_element_type=jnp.float32,
    )
    upvals = jnp.dot(
        normed,
        lax.all_gather(up_weight, "sp", axis=0, tiled=True),
        preferred_element_type=jnp.float32,
    )
    full_down = lax.all_gather(down_weight, "sp", axis=1, tiled=True)
    hidden = (jax.nn.silu(gate) * upvals).astype(jnp.bfloat16)
    picked = hidden
    ffn = lax.psum_scatter(
        jnp.dot(picked, full_down, preferred_element_type=jnp.float32).astype(jnp.bfloat16),
        "tp",
        scatter_dimension=0,
        tiled=True,
    ).astype(jnp.float32)
    return (rows_mid.astype(jnp.float32) + ffn).astype(jnp.bfloat16)


MESH = pl.DeviceIdType.MESH
XS = 2
CS = 2
F32 = jnp.float32
BF16 = jnp.bfloat16


def dot_nt(a, b):
    return lax.dot_general(a, b, (((1,), (1,)), ((), ())), preferred_element_type=F32)


def dot_nn(a, b):
    return lax.dot_general(a, b, (((1,), (0,)), ((), ())), preferred_element_type=F32)


def kernel(
    nz,
    nt,
    q_ref,
    k_ref,
    v_ref,
    g_ref,
    ld_ref,
    cos_ref,
    sin_ref,
    hg_ref,
    res_ref,
    mg_ref,
    ow_hbm,
    gw_hbm,
    uw_hbm,
    dw_hbm,
    out_ref,
    ow,
    w,
    qrot,
    inner,
    cumx,
    contrib,
    c_out,
    t_out,
    c_in,
    t_in,
    p_out,
    tt_out,
    p_in,
    tt_in,
    retained,
    mix_out,
    mix_in,
    middle,
    norm_own,
    normed,
    keep,
    s1,
    r1,
    s2,
    r2,
    s3,
    r3,
    ow_sem,
    own_sem,
    w_send,
    w_recv,
    f_send,
    f_recv,
    cx_send,
    cx_recv,
    pz_send,
    pz_recv,
    mix_send,
    mix_recv,
    nz_send,
    nz_recv,
    nt_send,
    nt_recv,
    t1_send,
    t1_recv,
    t2_send,
    t2_recv,
    t3_send,
    t3_recv,
):
    sp = lax.axis_index("sp")
    tp = lax.axis_index("tp")
    z, x = sp // XS, lax.rem(sp, XS)
    y, c = tp // CS, lax.rem(tp, CS)
    rows = q_ref.shape[0]
    heads = ld_ref.shape[1]
    hd = q_ref.shape[1] // heads
    quarter = rows // nt
    weights = (gw_hbm, uw_hbm, dw_hbm)
    x_peer = (z * XS + (1 - x), tp)
    c_peer = (sp, y * CS + (1 - c))
    y_peer = (sp, (1 - y) * CS + c)

    def z_at(d):
        return lax.rem(z + d, nz)

    def z_peer(d):
        return (z_at(d) * XS + x, tp)

    def t_at(d):
        return lax.rem(tp + d, nt)

    def t_peer(d):
        return (sp, t_at(d))

    def remote(src, dst, send, recv, peer):
        return pltpu.make_async_remote_copy(
            src_ref=src,
            dst_ref=dst,
            send_sem=send,
            recv_sem=recv,
            device_id=peer,
            device_id_type=MESH,
        )

    started = []

    def go(copy):
        copy.start()
        started.append(copy)
        return copy

    ow_copy = pltpu.make_async_copy(ow_hbm, ow, ow_sem)
    ow_copy.start()
    own_copies = []
    for m in range(3):
        own = pltpu.make_async_copy(weights[m].at[z], w.at[m, sp], own_sem.at[m])
        own.start()
        own_copies.append(own)

    barrier = pltpu.get_barrier_semaphore()
    peers = [z_peer(d) for d in range(1, nz)] + [x_peer] + [t_peer(d) for d in range(1, nt)]
    for peer in peers:
        pl.semaphore_signal(barrier, inc=1, device_id=peer, device_id_type=MESH)
    pl.semaphore_wait(barrier, len(peers))

    w_copies = {}

    def send_weight(m, d):
        w_copies[m, d] = go(
            remote(
                weights[m].at[z_at(d)], w.at[m, sp], w_send.at[m, d], w_recv.at[m, d], z_peer(d)
            )
        )

    f_copies = {}

    def forward(m, d):
        slot = lax.rem(z - d + nz, nz) * XS + x
        if d == 0:
            own_copies[m].wait()
        else:
            w_copies[m, d].wait_recv()
        f_copies[m, d] = go(
            remote(w.at[m, slot], w.at[m, slot], f_send.at[m, d], f_recv.at[m, d], x_peer)
        )

    send_weight(0, 2 % nz)

    ti = lax.broadcasted_iota(jnp.int32, (rows, rows), 0)
    si = lax.broadcasted_iota(jnp.int32, (rows, rows), 1)
    lower = si <= ti
    cumul = lax.dot_general(
        lower.astype(F32),
        ld_ref[...],
        (((1,), (0,)), ((), ())),
        precision=lax.Precision.HIGHEST,
        preferred_element_type=F32,
    )
    cos, sin = cos_ref[...], sin_ref[...]
    for h in range(heads):
        cols = slice(h * hd, (h + 1) * hd)
        qf = q_ref[:, cols].astype(F32)
        kf = k_ref[:, cols].astype(F32)
        vb = v_ref[:, cols]
        qb = (qf * cos + pltpu.roll(qf, hd // 2, 1) * sin).astype(BF16)
        kb = ((kf * cos + pltpu.roll(kf, hd // 2, 1) * sin) * hd ** (-0.5)).astype(BF16)
        cum = jnp.broadcast_to(cumul[:, h : h + 1], (rows, rows))
        spread = cum - jnp.transpose(cum)
        weight = jnp.where(lower, jnp.exp(jnp.where(lower, spread, 0.0)), 0.0)
        probs = (dot_nt(qb, kb) * weight).astype(BF16)
        inner[:, cols] = dot_nn(probs, vb)
        last = cum[rows - 1 :, :]
        kw = kb.astype(F32) * jnp.exp(last - cum)
        cb = dot_nn(jnp.transpose(kw).astype(BF16), vb)
        contrib[h] = cb
        c_out[h] = cb.astype(BF16)
        t_out[h : h + 1, :] = jnp.exp(last)
        qrot[:, cols] = qb.astype(F32)
        cumx[:, cols] = jnp.exp(cum)
    cx = go(remote(c_out, c_in, cx_send.at[0], cx_recv.at[0], x_peer))
    tx = go(remote(t_out, t_in, cx_send.at[1], cx_recv.at[1], x_peer))
    forward(0, 0)
    cx.wait_recv()
    tx.wait_recv()
    first = x == 0
    for h in range(heads):
        own_c, own_t = contrib[h], t_out[h : h + 1, :]
        other_c, other_t = c_in[h].astype(F32), t_in[h : h + 1, :]
        plane = jnp.where(first, other_t * own_c + other_c, own_t * other_c + own_c)
        p_out[h] = plane.astype(BF16)
        tt_out[h : h + 1, :] = own_t * other_t
    pz, tz = {}, {}
    for d in range(1, nz):
        pz[d] = go(remote(p_out, p_in.at[z], pz_send.at[0, d], pz_recv.at[0, d], z_peer(d)))
        tz[d] = go(remote(tt_out, tt_in.at[z], pz_send.at[1, d], pz_recv.at[1, d], z_peer(d)))
    for m in range(3):
        for d in range(1, nz):
            if (m, d) not in w_copies:
                send_weight(m, d)
    forward(1, 0)
    forward(2, 0)
    for d in range(1, nz):
        pz[d].wait_recv()
        tz[d].wait_recv()
    p_in[z] = p_out[...]
    tt_in[z] = tt_out[...]
    for h in range(heads):
        cols = slice(h * hd, (h + 1) * hd)
        state = jnp.zeros((hd, hd), F32)
        for zz in range(nz - 1):
            later = tt_in[zz, h : h + 1, :] * state + p_in[zz, h].astype(F32)
            state = jnp.where(zz < z, later, state)
        state = jnp.where(first, state, t_in[h : h + 1, :] * state + c_in[h].astype(F32))
        cross = lax.dot_general(
            qrot[:, cols],
            state,
            (((1,), (0,)), ((), ())),
            precision=lax.Precision.HIGHEST,
            preferred_element_type=F32,
        )
        ret = inner[:, cols] + cumx[:, cols] * cross
        scale = lax.rsqrt(jnp.mean(ret * ret, axis=-1, keepdims=True) + EPS)
        gf = g_ref[:, cols].astype(F32)
        retained[:, cols] = (
            ret * scale * hg_ref[:, cols] * (gf / (1.0 + jnp.exp(-gf)))
        ).astype(BF16)
    ow_copy.wait()
    for d in list(range(1, nt)) + [0]:
        mine = pl.multiple_of(t_at(d) * quarter, quarter)
        part = dot_nn(retained[pl.ds(mine, quarter), :], ow[...]).astype(BF16)
        if d == 0:
            mix_in[tp] = part
        else:
            mix_out[d] = part
            go(
                remote(
                    mix_out.at[d], mix_in.at[tp], mix_send.at[d], mix_recv.at[d], t_peer(d)
                )
            )
    for d in range(1, nt):
        remote(
            mix_out.at[d], mix_in.at[tp], mix_send.at[d], mix_recv.at[d], t_peer(d)
        ).wait_recv()
    mixed = mix_in[0].astype(F32)
    for j in range(1, nt):
        mixed += mix_in[j].astype(F32)
    mine = pl.multiple_of(tp * quarter, quarter)
    mid = (res_ref[pl.ds(mine, quarter), :].astype(F32) + mixed).astype(BF16).astype(F32)
    middle[...] = mid
    norm_own[...] = (
        mid * lax.rsqrt(jnp.mean(mid * mid, axis=-1, keepdims=True) + EPS) * mg_ref[...]
    ).astype(BF16)
    normed[z, tp] = norm_own[...]
    ncopy = {}
    for d in range(1, nz):
        ncopy[d] = go(
            remote(norm_own, normed.at[z, tp], nz_send.at[d], nz_recv.at[d], z_peer(d))
        )
    tcopy = {}
    for e in range(1, nt):
        tcopy[0, e] = go(
            remote(norm_own, normed.at[z, tp], nt_send.at[0, e], nt_recv.at[0, e], t_peer(e))
        )
    order = [2 % nz] + [d for d in range(1, nz) if d != 2 % nz]
    for d in order:
        forward(0, d)
    for m in (1, 2):
        for d in range(1, nz):
            forward(m, d)
    for d in range(1, nz):
        ncopy[d].wait_recv()
        zz = lax.rem(z - d + nz, nz)
        for e in range(1, nt):
            tcopy[d, e] = go(
                remote(
                    normed.at[zz, tp],
                    normed.at[zz, tp],
                    nt_send.at[d, e],
                    nt_recv.at[d, e],
                    t_peer(e),
                )
            )
    for key in sorted(f_copies):
        f_copies[key].wait_recv()
    for key in sorted(tcopy):
        tcopy[key].wait_recv()

    ns = nz * XS
    width = w.shape[3]
    t1, t2 = {}, {}
    chunks = [d for d in (2, 1, 3) if d < nz] + list(range(4, nz)) + [0]

    def compute(d):
        zz = z_at(d)
        block = normed[zz].reshape(rows, normed.shape[3])
        gate = dot_nt(block[:, :width], w[0, 0])
        up = dot_nt(block[:, :width], w[1, 0])
        for s in range(1, ns):
            piece = block[:, s * width : (s + 1) * width]
            gate += dot_nt(piece, w[0, s])
            up += dot_nt(piece, w[1, s])
        hidden = (gate / (1.0 + jnp.exp(-gate)) * up).astype(BF16)
        low = c == 0
        for s in range(ns):
            part = dot_nn(hidden, w[2, s])
            cols = slice(s * width, (s + 1) * width)
            for yy in range(nt // CS):
                even = part[(yy * CS) * quarter : (yy * CS + 1) * quarter]
                odd = part[(yy * CS + 1) * quarter : (yy * CS + 2) * quarter]
                keep[d, yy, :, cols] = jnp.where(low, even, odd)
                s1[d, yy, :, cols] = jnp.where(low, odd, even).astype(BF16)
        t1[d] = go(remote(s1.at[d], r1.at[d], t1_send.at[d], t1_recv.at[d], c_peer))

    def second(d):
        t1[d].wait_recv()
        s2[d] = (keep[d, 1 - y] + r1[d, 1 - y].astype(F32)).astype(BF16)
        t2[d] = go(remote(s2.at[d], r2.at[d], t2_send.at[d], t2_recv.at[d], y_peer))
        keep[d, y] = keep[d, y] + r1[d, y].astype(F32)

    t3 = {}

    def third(d):
        t2[d].wait_recv()
        total = keep[d, y] + r2[d].astype(F32)
        if d == 0:
            middle[...] = middle[...] + total
        else:
            s3[d] = total.astype(BF16)
            t3[d] = go(remote(s3.at[d], r3.at[d], t3_send.at[d], t3_recv.at[d], z_peer(d)))

    count = len(chunks)
    for step in range(count + 2):
        if step < count:
            compute(chunks[step])
        if 1 <= step < count + 1:
            second(chunks[step - 1])
        if step >= 2:
            third(chunks[step - 2])
    total = middle[...]
    for d in range(1, nz):
        t3[d].wait_recv()
        total += r3[d].astype(F32)
    out_ref[...] = total.astype(BF16)
    for copy in started:
        copy.wait_send()


def fast_body(
    queries,
    key_rows,
    value_rows,
    gate_input,
    log_decay,
    head_gain,
    out_weight,
    residual,
    mlp_gain,
    gate_weight,
    up_weight,
    down_weight,
):
    rows, wide = queries.shape
    heads = log_decay.shape[1]
    hd = wide // heads
    model = residual.shape[1]
    ns, nt = lax.axis_size("sp"), lax.axis_size("tp")
    nz = ns // XS
    quarter = rows // nt
    width, units = gate_weight.shape
    share = units // nz
    offset = lax.axis_index("sp") * rows
    positions = (offset + lax.iota(jnp.int32, rows)).astype(F32)[:, None]
    half = hd // 2
    freq = 10000.0 ** (-jnp.linspace(0.0, 1.0, half, dtype=F32))
    angles = positions * freq
    cos, sin = jnp.cos(angles), jnp.sin(angles)
    cos = jnp.concatenate([cos, cos], axis=1)
    sin = jnp.concatenate([-sin, sin], axis=1)
    gw = gate_weight.T.reshape(nz, share, width)
    uw = up_weight.T.reshape(nz, share, width)
    dw = down_weight.reshape(nz, share, width)
    vmem = pl.BlockSpec(memory_space=pltpu.VMEM)
    anyspace = pl.BlockSpec(memory_space=pl.ANY)
    dma = pltpu.SemaphoreType.DMA
    scratch = [
        pltpu.VMEM(out_weight.shape, BF16),
        pltpu.VMEM((3, ns, share, width), BF16),
        pltpu.VMEM((rows, wide), F32),
        pltpu.VMEM((rows, wide), F32),
        pltpu.VMEM((rows, wide), F32),
        pltpu.VMEM((heads, hd, hd), F32),
        pltpu.VMEM((heads, hd, hd), BF16),
        pltpu.VMEM((heads, hd), F32),
        pltpu.VMEM((heads, hd, hd), BF16),
        pltpu.VMEM((heads, hd), F32),
        pltpu.VMEM((heads, hd, hd), BF16),
        pltpu.VMEM((heads, hd), F32),
        pltpu.VMEM((nz, heads, hd, hd), BF16),
        pltpu.VMEM((nz, heads, hd), F32),
        pltpu.VMEM((rows, wide), BF16),
        pltpu.VMEM((nt, quarter, model), BF16),
        pltpu.VMEM((nt, quarter, model), BF16),
        pltpu.VMEM((quarter, model), F32),
        pltpu.VMEM((quarter, model), BF16),
        pltpu.VMEM((nz, nt, quarter, model), BF16),
        pltpu.VMEM((nz, nt // CS, quarter, model), F32),
        pltpu.VMEM((nz, nt // CS, quarter, model), BF16),
        pltpu.VMEM((nz, nt // CS, quarter, model), BF16),
        pltpu.VMEM((nz, quarter, model), BF16),
        pltpu.VMEM((nz, quarter, model), BF16),
        pltpu.VMEM((nz, quarter, model), BF16),
        pltpu.VMEM((nz, quarter, model), BF16),
        dma,
        dma((3,)),
        dma((3, nz)),
        dma((3, nz)),
        dma((3, nz)),
        dma((3, nz)),
        dma((2,)),
        dma((2,)),
        dma((2, nz)),
        dma((2, nz)),
        dma((nt,)),
        dma((nt,)),
        dma((nz,)),
        dma((nz,)),
        dma((nz, nt)),
        dma((nz, nt)),
        dma((nz,)),
        dma((nz,)),
        dma((nz,)),
        dma((nz,)),
        dma((nz,)),
        dma((nz,)),
    ]
    return pl.pallas_call(
        functools.partial(kernel, nz, nt),
        out_shape=jax.ShapeDtypeStruct((quarter, model), BF16),
        in_specs=[vmem] * 10 + [anyspace] * 4,
        out_specs=vmem,
        scratch_shapes=scratch,
        compiler_params=pltpu.CompilerParams(
            collective_id=0, has_side_effects=True, vmem_limit_bytes=60 * 1024 * 1024
        ),
    )(
        queries,
        key_rows,
        value_rows,
        gate_input,
        log_decay,
        cos,
        sin,
        head_gain.reshape(1, wide),
        residual,
        mlp_gain.reshape(1, model),
        out_weight,
        gw,
        uw,
        dw,
    )


def fits(mesh, queries, log_decay, gate_weight):
    ns, nt = mesh.shape["sp"], mesh.shape["tp"]
    tokens, wide = queries.shape
    if ns % XS or ns // XS < 3 or nt != 2 * CS or tokens // ns != BLOCK:
        return False
    nz = ns // XS
    hidden = gate_weight.shape[1] // nt
    return (
        gate_weight.shape[0] // ns % 128 == 0
        and hidden % (16 * nz) == 0
        and wide // log_decay.shape[1] == 128
        and BLOCK % (16 * nt) == 0
    )


def solution(mesh):
    def run(*args):
        good = fits(mesh, args[0], args[4], args[9])
        return jax.shard_map(
            fast_body if good else body,
            mesh=mesh,
            in_specs=(
                P("sp", "tp"),
                P("sp", "tp"),
                P("sp", "tp"),
                P("sp", "tp"),
                P("sp", "tp"),
                P("tp"),
                P("tp", None),
                P("sp", None),
                P(),
                P("sp", "tp"),
                P("sp", "tp"),
                P("tp", "sp"),
            ),
            out_specs=P(("sp", "tp"), None),
            check_vma=False,
        )(*args)

    return run
```

```python
import functools
import math

import jax
import jax.numpy as jnp
from jax import lax
from jax.experimental import pallas as pl
from jax.experimental.pallas import tpu as pltpu
from jax.sharding import PartitionSpec as P

BLOCK = 128


EPS = 1e-06


def prefix_2(x, axis, join, neutral):
    place = lax.axis_index(axis)
    gathered = jax.tree.map(
        lambda a, kind: lax.all_gather(a.astype(kind), axis), x, (jnp.bfloat16, jnp.bfloat16)
    )
    state = jax.tree.map(lambda a, e: jnp.zeros_like(a) + jnp.asarray(e, a.dtype), x, neutral)

    def one(step, state):
        return join(
            state,
            jax.tree.map(
                lambda a, own: lax.dynamic_index_in_dim(a, step, 0, False).astype(own.dtype),
                gathered,
                x,
            ),
        )

    return lax.fori_loop(0, place, one, state)


def rotate(values_in, positions):
    half = values_in.shape[-1] // 2
    freq = 10000.0 ** (-jnp.linspace(0.0, 1.0, half, dtype=jnp.float32))
    angles = positions * freq
    angles = jnp.concatenate([angles, angles], axis=-1)
    first = values_in[..., :half]
    second = values_in[..., half:]
    turned = jnp.concatenate([-second, first], axis=-1)
    return values_in * jnp.cos(angles) + turned * jnp.sin(angles)


def row_norm(stream, gain):
    return stream * lax.rsqrt(jnp.mean(stream * stream, axis=-1, keepdims=True) + EPS) * gain


def join_states(earlier, later):
    return (earlier[0] * later[0], later[0][:, None, None] * earlier[1] + later[1])


def body(
    queries,
    key_rows,
    value_rows,
    gate_input,
    log_decay,
    head_gain,
    out_weight,
    residual,
    mlp_gain,
    gate_weight,
    up_weight,
    down_weight,
):
    tok_rows = queries.shape[0]
    heads_here = log_decay.shape[1]
    head_size = head_gain.shape[0] // heads_here
    quarter = tok_rows // lax.axis_size("tp")
    offset = lax.axis_index("sp") * tok_rows
    positions = (offset + lax.iota(jnp.int32, tok_rows)).astype(jnp.float32)[:, None, None]
    q_rot = rotate(
        queries.reshape(tok_rows, heads_here, head_size).astype(jnp.float32), positions
    ).astype(jnp.bfloat16)
    k_rot = (
        rotate(key_rows.reshape(tok_rows, heads_here, head_size).astype(jnp.float32), positions)
        * head_size ** (-0.5)
    ).astype(jnp.bfloat16)
    blocks = tok_rows // BLOCK
    q_blocks = q_rot.reshape(blocks, BLOCK, heads_here, head_size)
    k_blocks = k_rot.reshape(blocks, BLOCK, heads_here, head_size)
    v_blocks = value_rows.reshape(blocks, BLOCK, heads_here, head_size)
    cumul = jnp.cumsum(log_decay.reshape(blocks, BLOCK, heads_here), axis=1)
    by_head = cumul.transpose(0, 2, 1)
    lower = jnp.tril(jnp.ones((BLOCK, BLOCK), dtype=bool))
    spread = by_head[:, :, :, None] - by_head[:, :, None, :]
    weight = jnp.where(lower, jnp.exp(jnp.where(lower, spread, 0.0)), 0.0)
    scores = jnp.einsum("nthd,nshd->nhts", q_blocks, k_blocks, preferred_element_type=jnp.float32)
    probs = (scores * weight).astype(jnp.bfloat16)
    inner = jnp.einsum("nhts,nshe->nthe", probs, v_blocks, preferred_element_type=jnp.float32)
    k_weighted = (
        k_blocks.astype(jnp.float32) * jnp.exp(cumul[:, -1:, :] - cumul)[..., None]
    ).astype(jnp.bfloat16)
    contrib = jnp.einsum(
        "nshd,nshe->nhde", k_weighted, v_blocks, preferred_element_type=jnp.float32
    )
    totals = jnp.exp(cumul[:, -1, :])

    def advance(carry, items):
        state, prefix = carry
        factor, update = items
        return ((state * factor[:, None, None] + update, prefix * factor), (state, prefix))

    start_state = jnp.zeros((heads_here, head_size, head_size), jnp.float32)
    start_prefix = jnp.ones((heads_here,), jnp.float32)
    (dev_state, dev_total), (local_before, prefixes) = lax.scan(
        advance, (start_state, start_prefix), (totals, contrib)
    )
    _, incoming = prefix_2((dev_total, dev_state), "sp", join_states, (start_prefix, start_state))
    before = local_before + prefixes[:, :, None, None] * incoming[None]
    cross = jnp.einsum(
        "nthd,nhde->nthe", q_blocks.astype(jnp.float32), before, precision=lax.Precision.HIGHEST
    )
    cross = cross * jnp.exp(cumul)[..., None]
    result = (inner + cross).reshape(tok_rows, heads_here, head_size)
    result = row_norm(result, head_gain.reshape(heads_here, head_size)).reshape(
        tok_rows, heads_here * head_size
    )
    retained = (result * jax.nn.silu(gate_input.astype(jnp.float32))).astype(jnp.bfloat16)
    picked = retained
    mixed = lax.psum_scatter(
        jnp.dot(picked, out_weight, preferred_element_type=jnp.float32).astype(jnp.bfloat16),
        "tp",
        scatter_dimension=0,
        tiled=True,
    ).astype(jnp.float32)
    own_rows = lax.dynamic_slice_in_dim(residual, lax.axis_index("tp") * quarter, quarter, 0)
    rows_mid = (own_rows.astype(jnp.float32) + mixed).astype(jnp.bfloat16)
    own_normed = row_norm(rows_mid.astype(jnp.float32), mlp_gain).astype(jnp.bfloat16)
    normed = lax.all_gather(own_normed, "tp", axis=0, tiled=True)
    gate = jnp.dot(
        normed,
        lax.all_gather(gate_weight, "sp", axis=0, tiled=True),
        preferred_element_type=jnp.float32,
    )
    upvals = jnp.dot(
        normed,
        lax.all_gather(up_weight, "sp", axis=0, tiled=True),
        preferred_element_type=jnp.float32,
    )
    full_down = lax.all_gather(down_weight, "sp", axis=1, tiled=True)
    hidden = (jax.nn.silu(gate) * upvals).astype(jnp.bfloat16)
    picked = hidden
    ffn = lax.psum_scatter(
        jnp.dot(picked, full_down, preferred_element_type=jnp.float32).astype(jnp.bfloat16),
        "tp",
        scatter_dimension=0,
        tiled=True,
    ).astype(jnp.float32)
    return (rows_mid.astype(jnp.float32) + ffn).astype(jnp.bfloat16)


MESH = pl.DeviceIdType.MESH
XS = 2
CS = 2
F32 = jnp.float32
BF16 = jnp.bfloat16


def dot_nt(a, b):
    return lax.dot_general(a, b, (((1,), (1,)), ((), ())), preferred_element_type=F32)


def dot_nn(a, b):
    return lax.dot_general(a, b, (((1,), (0,)), ((), ())), preferred_element_type=F32)


def kernel(
    nz,
    nt,
    q_ref,
    k_ref,
    v_ref,
    g_ref,
    ld_ref,
    hg_ref,
    res_ref,
    mg_ref,
    ow_hbm,
    gw_hbm,
    uw_hbm,
    dw_hbm,
    out_ref,
    ow,
    raw,
    turned,
    w,
    qrot,
    inner,
    cumx,
    contrib,
    c_out,
    t_out,
    c_in,
    t_in,
    p_out,
    tt_out,
    p_in,
    tt_in,
    s_own,
    s_out,
    s_in,
    retained,
    mix_out,
    mix_in,
    acc,
    norm_own,
    normed,
    hidden,
    keep,
    s1,
    r1,
    s2,
    r2,
    s3,
    r3,
    ow_sem,
    raw_sem,
    own_sem,
    w_send,
    w_recv,
    f_send,
    f_recv,
    cx_send,
    cx_recv,
    pz_send,
    pz_recv,
    sx_send,
    sx_recv,
    mix_send,
    mix_recv,
    nz_send,
    nz_recv,
    nt_send,
    nt_recv,
    t1_send,
    t1_recv,
    t2_send,
    t2_recv,
    t3_send,
    t3_recv,
):
    sp = lax.axis_index("sp")
    tp = lax.axis_index("tp")
    z, x = sp // XS, lax.rem(sp, XS)
    y, c = tp // CS, lax.rem(tp, CS)
    rows = q_ref.shape[0]
    heads = ld_ref.shape[0]
    hh = heads // XS
    hd = q_ref.shape[1] // heads
    quarter = rows // nt
    share, width = w.shape[2], w.shape[3]
    group = XS * width
    x_peer = (z * XS + (1 - x), tp)
    c_peer = (sp, y * CS + (1 - c))
    y_peer = (sp, (1 - y) * CS + c)

    def z_at(d):
        return lax.rem(z + d, nz)

    def z_from(d):
        return lax.rem(z - d + nz, nz)

    def z_peer(d):
        return (z_at(d) * XS + x, tp)

    def t_at(d):
        return lax.rem(tp + d, nt)

    def t_peer(d):
        return (sp, t_at(d))

    def remote(src, dst, send, recv, peer):
        return pltpu.make_async_remote_copy(
            src_ref=src,
            dst_ref=dst,
            send_sem=send,
            recv_sem=recv,
            device_id=peer,
            device_id_type=MESH,
        )

    started = []

    def go(copy):
        copy.start()
        started.append(copy)
        return copy

    def piece(m, zz):
        at = pl.ds(pl.multiple_of(zz * share, 16), share)
        return dw_hbm.at[at] if m == 2 else turned.at[m, at]

    raw_copies = []
    for m, source in enumerate((gw_hbm, uw_hbm)):
        raw_copy = pltpu.make_async_copy(source, raw.at[m], raw_sem.at[m])
        raw_copy.start()
        raw_copies.append(raw_copy)
    ow_copy = pltpu.make_async_copy(ow_hbm, ow, ow_sem)
    own_copies = {}

    def take_own(m):
        own_copies[m] = pltpu.make_async_copy(piece(m, z), w.at[m, sp], own_sem.at[m])
        own_copies[m].start()

    take_own(2)
    ow_copy.start()

    barrier = pltpu.get_barrier_semaphore()
    peers = [z_peer(d) for d in range(1, nz)] + [x_peer] + [t_peer(d) for d in range(1, nt)]
    for peer in peers:
        pl.semaphore_signal(barrier, inc=1, device_id=peer, device_id_type=MESH)
    pl.semaphore_wait(barrier, len(peers))

    w_copies = {}

    def send_weight(m, d):
        w_copies[m, d] = go(
            remote(piece(m, z_at(d)), w.at[m, sp], w_send.at[m, d], w_recv.at[m, d], z_peer(d))
        )

    f_copies = {}

    def forward(m, d):
        slot = z_from(d) * XS + x
        if d == 0:
            own_copies[m].wait()
        else:
            w_copies[m, d].wait_recv()
        f_copies[m, d] = go(
            remote(w.at[m, slot], w.at[m, slot], f_send.at[m, d], f_recv.at[m, d], x_peer)
        )

    far = 2
    near = [d for d in range(1, nz) if d != far]
    send_weight(2, far)

    ti = lax.broadcasted_iota(jnp.int32, (rows, rows), 0)
    si = lax.broadcasted_iota(jnp.int32, (rows, rows), 1)
    lower = si <= ti
    cumul = lax.dot_general(
        ld_ref[...],
        (ti <= si).astype(F32),
        (((1,), (0,)), ((), ())),
        precision=lax.Precision.HIGHEST,
        preferred_element_type=F32,
    )
    half = hd // 2
    lane = lax.broadcasted_iota(jnp.int32, (1, hd), 1)
    low_half = lane < half
    index = jnp.where(low_half, lane, lane - half).astype(F32)
    freq = jnp.exp(index * (-math.log(10000.0) / (half - 1)))
    angles = (sp * rows + lax.broadcasted_iota(jnp.int32, (rows, hd), 0)).astype(F32) * freq
    cos = jnp.cos(angles)
    sin = jnp.sin(angles)
    sin = jnp.where(low_half, -sin, sin)
    for h in range(heads):
        cols = slice(h * hd, (h + 1) * hd)
        qf = q_ref[:, cols].astype(F32)
        kf = k_ref[:, cols].astype(F32)
        vb = v_ref[:, cols]
        qb = (qf * cos + pltpu.roll(qf, half, 1) * sin).astype(BF16)
        kb = ((kf * cos + pltpu.roll(kf, half, 1) * sin) * hd ** (-0.5)).astype(BF16)
        along = jnp.broadcast_to(cumul[h : h + 1, :], (rows, rows))
        cum = jnp.transpose(along)
        spread = cum - along
        weight = jnp.where(lower, jnp.exp(jnp.where(lower, spread, 0.0)), 0.0)
        probs = (dot_nt(qb, kb) * weight).astype(BF16)
        inner[:, cols] = dot_nn(probs, vb)
        last = cum[rows - 1 :, :]
        kw = kb.astype(F32) * jnp.exp(last - cum)
        cb = dot_nn(jnp.transpose(kw).astype(BF16), vb)
        contrib[h] = cb
        c_out[h] = cb.astype(BF16)
        t_out[h] = jnp.broadcast_to(jnp.exp(last), t_out.shape[1:])
        qrot[:, cols] = qb.astype(F32)
        cumx[:, cols] = jnp.exp(cum)
    mine_h, other_h = x * hh, (1 - x) * hh
    cx = go(remote(c_out.at[pl.ds(other_h, hh)], c_in, cx_send.at[0], cx_recv.at[0], x_peer))
    tx = go(remote(t_out, t_in, cx_send.at[1], cx_recv.at[1], x_peer))
    forward(2, 0)
    for m in range(2):
        raw_copies[m].wait()
        for j in range(raw.shape[2] // 128):
            turned[m, j * 128 : (j + 1) * 128, :] = jnp.transpose(
                raw[m, :, j * 128 : (j + 1) * 128]
            )
        take_own(m)
    cx.wait_recv()
    tx.wait_recv()
    first = x == 0
    for i in range(hh):
        own_c, own_t = contrib[mine_h + i], t_out[mine_h + i][:1]
        other_c, other_t = c_in[i].astype(F32), t_in[mine_h + i][:1]
        plane = jnp.where(first, other_t * own_c + other_c, own_t * other_c + own_c)
        p_out[i] = plane.astype(BF16)
        tt_out[i] = jnp.broadcast_to(own_t * other_t, tt_out.shape[1:])
    pz, tz = {}, {}
    for d in range(1, nz):
        pz[d] = go(remote(p_out, p_in.at[z], pz_send.at[0, d], pz_recv.at[0, d], z_peer(d)))
        tz[d] = go(remote(tt_out, tt_in.at[z], pz_send.at[1, d], pz_recv.at[1, d], z_peer(d)))
    for d in [far] + near:
        send_weight(0, d)
    send_weight(1, far)
    forward(0, 0)
    for d in range(1, nz):
        pz[d].wait_recv()
        tz[d].wait_recv()
    p_in[z] = p_out[...]
    tt_in[z] = tt_out[...]
    for i in range(hh):
        state = jnp.zeros((hd, hd), F32)
        for zz in range(nz - 1):
            later = tt_in[zz, i][:1] * state + p_in[zz, i].astype(F32)
            state = jnp.where(zz < z, later, state)
        early_t = jnp.where(first, t_out[mine_h + i][:1], t_in[mine_h + i][:1])
        early_c = jnp.where(first, contrib[mine_h + i], c_in[i].astype(F32))
        after = early_t * state + early_c
        s_own[i] = jnp.where(first, state, after)
        s_out[i] = jnp.where(first, after, state).astype(BF16)
    sx = go(remote(s_out, s_in, sx_send, sx_recv, x_peer))
    forward(1, 0)
    forward(2, far)

    def finish(h, state, cols):
        cross = lax.dot_general(
            qrot[:, cols],
            state,
            (((1,), (0,)), ((), ())),
            precision=lax.Precision.HIGHEST,
            preferred_element_type=F32,
        )
        ret = inner[:, cols] + cumx[:, cols] * cross
        scale = lax.rsqrt(jnp.mean(ret * ret, axis=-1, keepdims=True) + EPS)
        gf = g_ref[:, cols].astype(F32)
        retained[:, cols] = (
            ret * scale * hg_ref[:, cols] * (gf / (1.0 + jnp.exp(-gf)))
        ).astype(BF16)

    sx.wait_recv()
    for h in range(heads):
        cols = slice(h * hd, (h + 1) * hd)
        i = h % hh
        mine = x == h // hh
        finish(h, jnp.where(mine, s_own[i], s_in[i].astype(F32)), cols)
    ow_copy.wait()
    mixes = []
    for d in list(range(1, nt)) + [0]:
        mine = pl.multiple_of(t_at(d) * quarter, quarter)
        part = dot_nn(retained[pl.ds(mine, quarter), :], ow[...]).astype(BF16)
        if d == 0:
            mix_in[tp] = part
        else:
            mix_out[d] = part
            mixes.append(
                go(
                    remote(
                        mix_out.at[d], mix_in.at[tp], mix_send.at[d], mix_recv.at[d], t_peer(d)
                    )
                )
            )
    forward(0, far)
    for mix in mixes:
        mix.wait_recv()
    mixed = mix_in[0].astype(F32)
    for j in range(1, nt):
        mixed += mix_in[j].astype(F32)
    mine = pl.multiple_of(tp * quarter, quarter)
    mid = (res_ref[pl.ds(mine, quarter), :].astype(F32) + mixed).astype(BF16).astype(F32)
    for g in range(nz):
        acc[g] = mid[:, g * group : (g + 1) * group]
    norm_own[...] = (
        mid * lax.rsqrt(jnp.mean(mid * mid, axis=-1, keepdims=True) + EPS) * mg_ref[...]
    ).astype(BF16)
    normed[z, tp] = norm_own[...]
    ncopy, tcopy = {}, {}
    for d in [far] + near:
        ncopy[d] = go(
            remote(norm_own, normed.at[z, tp], nz_send.at[d], nz_recv.at[d], z_peer(d))
        )
    for e in range(1, nt):
        tcopy[0, e] = go(
            remote(norm_own, normed.at[z, tp], nt_send.at[0, e], nt_recv.at[0, e], t_peer(e))
        )
    for d in near:
        send_weight(1, d)
    for d in near:
        send_weight(2, d)
    for d in near:
        forward(0, d)
    forward(1, far)
    for d in [far] + near:
        ncopy[d].wait_recv()
        zz = z_from(d)
        for e in range(1, nt):
            tcopy[d, e] = go(
                remote(
                    normed.at[zz, tp],
                    normed.at[zz, tp],
                    nt_send.at[d, e],
                    nt_recv.at[d, e],
                    t_peer(e),
                )
            )
    for d in near:
        forward(1, d)
    for d in range(nz):
        f_copies[0, d].wait_recv()
        f_copies[1, d].wait_recv()
    for key in sorted(tcopy):
        tcopy[key].wait_recv()

    ns = nz * XS
    for zz in range(nz):
        block = normed[zz].reshape(rows, normed.shape[3])
        gate = dot_nt(block[:, :width], w[0, 0])
        up = dot_nt(block[:, :width], w[1, 0])
        for s in range(1, ns):
            cut = block[:, s * width : (s + 1) * width]
            gate += dot_nt(cut, w[0, s])
            up += dot_nt(cut, w[1, s])
        hidden[zz * rows : (zz + 1) * rows, :] = (
            gate / (1.0 + jnp.exp(-gate)) * up
        ).astype(BF16)

    t1, t2, t3 = {}, {}, {}
    low = c == 0

    def compute(b):
        if b in near:
            forward(2, b)
        f_copies[2, b].wait_recv()
        for u in range(XS):
            part = dot_nn(hidden[...], w[2, z_from(b) * XS + u])
            cols = slice(u * width, (u + 1) * width)
            for zz in range(nz):
                for yy in range(nt // CS):
                    at = zz * rows + yy * CS * quarter
                    even = part[at : at + quarter]
                    odd = part[at + quarter : at + 2 * quarter]
                    keep[b, yy, zz, :, cols] = jnp.where(low, even, odd)
                    s1[b, yy, zz, :, cols] = jnp.where(low, odd, even).astype(BF16)
        t1[b] = go(remote(s1.at[b], r1.at[b], t1_send.at[b], t1_recv.at[b], c_peer))

    def second(b):
        t1[b].wait_recv()
        s2[b] = (keep[b, 1 - y] + r1[b, 1 - y].astype(F32)).astype(BF16)
        t2[b] = go(remote(s2.at[b], r2.at[b], t2_send.at[b], t2_recv.at[b], y_peer))
        keep[b, y] = keep[b, y] + r1[b, y].astype(F32)

    def third(b):
        t2[b].wait_recv()
        for e in [far] + near:
            zz = z_at(e)
            s3[b, e] = (keep[b, y, zz] + r2[b, zz].astype(F32)).astype(BF16)
            t3[b, e] = go(
                remote(s3.at[b, e], r3.at[b, e], t3_send.at[b, e], t3_recv.at[b, e], z_peer(e))
            )
        g = z_from(b)
        acc[g] = acc[g] + keep[b, y, z] + r2[b, z].astype(F32)

    batches = [0, far] + near
    count = len(batches)
    for step in range(count + 2):
        if step < count:
            compute(batches[step])
        if 1 <= step < count + 1:
            second(batches[step - 1])
        if step >= 2:
            third(batches[step - 2])
    for b in batches:
        for e in [far] + near:
            t3[b, e].wait_recv()
            g = lax.rem(z - e - b + 2 * nz, nz)
            acc[g] = acc[g] + r3[b, e].astype(F32)
    for g in range(nz):
        out_ref[:, g * group : (g + 1) * group] = acc[g].astype(BF16)
    for copy in started:
        copy.wait_send()


def fast_body(
    queries,
    key_rows,
    value_rows,
    gate_input,
    log_decay,
    head_gain,
    out_weight,
    residual,
    mlp_gain,
    gate_weight,
    up_weight,
    down_weight,
):
    rows, wide = queries.shape
    heads = log_decay.shape[1]
    hd = wide // heads
    model = residual.shape[1]
    ns, nt = lax.axis_size("sp"), lax.axis_size("tp")
    nz = ns // XS
    quarter = rows // nt
    width, units = gate_weight.shape
    share = units // nz
    group = XS * width
    hh = heads // XS
    vmem = pl.BlockSpec(memory_space=pltpu.VMEM)
    anyspace = pl.BlockSpec(memory_space=pl.ANY)
    dma = pltpu.SemaphoreType.DMA
    scratch = [
        pltpu.VMEM(out_weight.shape, BF16),
        pltpu.VMEM((2, width, units), BF16),
        pltpu.VMEM((2, units, width), BF16),
        pltpu.VMEM((3, ns, share, width), BF16),
        pltpu.VMEM((rows, wide), F32),
        pltpu.VMEM((rows, wide), F32),
        pltpu.VMEM((rows, wide), F32),
        pltpu.VMEM((heads, hd, hd), F32),
        pltpu.VMEM((heads, hd, hd), BF16),
        pltpu.VMEM((heads, 8, hd), F32),
        pltpu.VMEM((hh, hd, hd), BF16),
        pltpu.VMEM((heads, 8, hd), F32),
        pltpu.VMEM((hh, hd, hd), BF16),
        pltpu.VMEM((hh, 8, hd), F32),
        pltpu.VMEM((nz, hh, hd, hd), BF16),
        pltpu.VMEM((nz, hh, 8, hd), F32),
        pltpu.VMEM((hh, hd, hd), F32),
        pltpu.VMEM((hh, hd, hd), BF16),
        pltpu.VMEM((hh, hd, hd), BF16),
        pltpu.VMEM((rows, wide), BF16),
        pltpu.VMEM((nt, quarter, model), BF16),
        pltpu.VMEM((nt, quarter, model), BF16),
        pltpu.VMEM((nz, quarter, group), F32),
        pltpu.VMEM((quarter, model), BF16),
        pltpu.VMEM((nz, nt, quarter, model), BF16),
        pltpu.VMEM((nz * rows, share), BF16),
        pltpu.VMEM((nz, nt // CS, nz, quarter, group), F32),
        pltpu.VMEM((nz, nt // CS, nz, quarter, group), BF16),
        pltpu.VMEM((nz, nt // CS, nz, quarter, group), BF16),
        pltpu.VMEM((nz, nz, quarter, group), BF16),
        pltpu.VMEM((nz, nz, quarter, group), BF16),
        pltpu.VMEM((nz, nz, quarter, group), BF16),
        pltpu.VMEM((nz, nz, quarter, group), BF16),
        dma,
        dma((2,)),
        dma((3,)),
        dma((3, nz)),
        dma((3, nz)),
        dma((3, nz)),
        dma((3, nz)),
        dma((2,)),
        dma((2,)),
        dma((2, nz)),
        dma((2, nz)),
        dma,
        dma,
        dma((nt,)),
        dma((nt,)),
        dma((nz,)),
        dma((nz,)),
        dma((nz, nt)),
        dma((nz, nt)),
        dma((nz,)),
        dma((nz,)),
        dma((nz,)),
        dma((nz,)),
        dma((nz, nz)),
        dma((nz, nz)),
    ]
    return pl.pallas_call(
        functools.partial(kernel, nz, nt),
        out_shape=jax.ShapeDtypeStruct((quarter, model), BF16),
        in_specs=[vmem] * 8 + [anyspace] * 4,
        out_specs=vmem,
        scratch_shapes=scratch,
        compiler_params=pltpu.CompilerParams(
            collective_id=0, has_side_effects=True, vmem_limit_bytes=60 * 1024 * 1024
        ),
    )(
        queries,
        key_rows,
        value_rows,
        gate_input,
        log_decay.T,
        head_gain.reshape(1, wide),
        residual,
        mlp_gain.reshape(1, model),
        out_weight,
        gate_weight,
        up_weight,
        down_weight,
    )


def fits(mesh, queries, log_decay, gate_weight):
    ns, nt = mesh.shape["sp"], mesh.shape["tp"]
    tokens, wide = queries.shape
    if ns % XS or ns // XS < 3 or nt != 2 * CS or tokens // ns != BLOCK:
        return False
    nz = ns // XS
    hidden = gate_weight.shape[1] // nt
    return (
        gate_weight.shape[0] // ns % 128 == 0
        and hidden % (16 * nz) == 0
        and wide // log_decay.shape[1] == 128
        and BLOCK % (16 * nt) == 0
        and hidden % 128 == 0
        and log_decay.shape[1] // nt % XS == 0
    )


def solution(mesh):
    def run(*args):
        good = fits(mesh, args[0], args[4], args[9])
        return jax.shard_map(
            fast_body if good else body,
            mesh=mesh,
            in_specs=(
                P("sp", "tp"),
                P("sp", "tp"),
                P("sp", "tp"),
                P("sp", "tp"),
                P("sp", "tp"),
                P("tp"),
                P("tp", None),
                P("sp", None),
                P(),
                P("sp", "tp"),
                P("sp", "tp"),
                P("tp", "sp"),
            ),
            out_specs=P(("sp", "tp"), None),
            check_vma=False,
        )(*args)

    return run
```

```python
import functools
import math

import jax
import jax.numpy as jnp
from jax import lax
from jax.experimental import pallas as pl
from jax.experimental.pallas import tpu as pltpu
from jax.sharding import PartitionSpec as P

BLOCK = 128


EPS = 1e-06


def prefix_2(x, axis, join, neutral):
    place = lax.axis_index(axis)
    gathered = jax.tree.map(
        lambda a, kind: lax.all_gather(a.astype(kind), axis), x, (jnp.bfloat16, jnp.bfloat16)
    )
    state = jax.tree.map(lambda a, e: jnp.zeros_like(a) + jnp.asarray(e, a.dtype), x, neutral)

    def one(step, state):
        return join(
            state,
            jax.tree.map(
                lambda a, own: lax.dynamic_index_in_dim(a, step, 0, False).astype(own.dtype),
                gathered,
                x,
            ),
        )

    return lax.fori_loop(0, place, one, state)


def rotate(values_in, positions):
    half = values_in.shape[-1] // 2
    freq = 10000.0 ** (-jnp.linspace(0.0, 1.0, half, dtype=jnp.float32))
    angles = positions * freq
    angles = jnp.concatenate([angles, angles], axis=-1)
    first = values_in[..., :half]
    second = values_in[..., half:]
    turned = jnp.concatenate([-second, first], axis=-1)
    return values_in * jnp.cos(angles) + turned * jnp.sin(angles)


def row_norm(stream, gain):
    return stream * lax.rsqrt(jnp.mean(stream * stream, axis=-1, keepdims=True) + EPS) * gain


def join_states(earlier, later):
    return (earlier[0] * later[0], later[0][:, None, None] * earlier[1] + later[1])


def body(
    queries,
    key_rows,
    value_rows,
    gate_input,
    log_decay,
    head_gain,
    out_weight,
    residual,
    mlp_gain,
    gate_weight,
    up_weight,
    down_weight,
):
    tok_rows = queries.shape[0]
    heads_here = log_decay.shape[1]
    head_size = head_gain.shape[0] // heads_here
    quarter = tok_rows // lax.axis_size("tp")
    offset = lax.axis_index("sp") * tok_rows
    positions = (offset + lax.iota(jnp.int32, tok_rows)).astype(jnp.float32)[:, None, None]
    q_rot = rotate(
        queries.reshape(tok_rows, heads_here, head_size).astype(jnp.float32), positions
    ).astype(jnp.bfloat16)
    k_rot = (
        rotate(key_rows.reshape(tok_rows, heads_here, head_size).astype(jnp.float32), positions)
        * head_size ** (-0.5)
    ).astype(jnp.bfloat16)
    blocks = tok_rows // BLOCK
    q_blocks = q_rot.reshape(blocks, BLOCK, heads_here, head_size)
    k_blocks = k_rot.reshape(blocks, BLOCK, heads_here, head_size)
    v_blocks = value_rows.reshape(blocks, BLOCK, heads_here, head_size)
    cumul = jnp.cumsum(log_decay.reshape(blocks, BLOCK, heads_here), axis=1)
    by_head = cumul.transpose(0, 2, 1)
    lower = jnp.tril(jnp.ones((BLOCK, BLOCK), dtype=bool))
    spread = by_head[:, :, :, None] - by_head[:, :, None, :]
    weight = jnp.where(lower, jnp.exp(jnp.where(lower, spread, 0.0)), 0.0)
    scores = jnp.einsum("nthd,nshd->nhts", q_blocks, k_blocks, preferred_element_type=jnp.float32)
    probs = (scores * weight).astype(jnp.bfloat16)
    inner = jnp.einsum("nhts,nshe->nthe", probs, v_blocks, preferred_element_type=jnp.float32)
    k_weighted = (
        k_blocks.astype(jnp.float32) * jnp.exp(cumul[:, -1:, :] - cumul)[..., None]
    ).astype(jnp.bfloat16)
    contrib = jnp.einsum(
        "nshd,nshe->nhde", k_weighted, v_blocks, preferred_element_type=jnp.float32
    )
    totals = jnp.exp(cumul[:, -1, :])

    def advance(carry, items):
        state, prefix = carry
        factor, update = items
        return ((state * factor[:, None, None] + update, prefix * factor), (state, prefix))

    start_state = jnp.zeros((heads_here, head_size, head_size), jnp.float32)
    start_prefix = jnp.ones((heads_here,), jnp.float32)
    (dev_state, dev_total), (local_before, prefixes) = lax.scan(
        advance, (start_state, start_prefix), (totals, contrib)
    )
    _, incoming = prefix_2((dev_total, dev_state), "sp", join_states, (start_prefix, start_state))
    before = local_before + prefixes[:, :, None, None] * incoming[None]
    cross = jnp.einsum(
        "nthd,nhde->nthe", q_blocks.astype(jnp.float32), before, precision=lax.Precision.HIGHEST
    )
    cross = cross * jnp.exp(cumul)[..., None]
    result = (inner + cross).reshape(tok_rows, heads_here, head_size)
    result = row_norm(result, head_gain.reshape(heads_here, head_size)).reshape(
        tok_rows, heads_here * head_size
    )
    retained = (result * jax.nn.silu(gate_input.astype(jnp.float32))).astype(jnp.bfloat16)
    picked = retained
    mixed = lax.psum_scatter(
        jnp.dot(picked, out_weight, preferred_element_type=jnp.float32).astype(jnp.bfloat16),
        "tp",
        scatter_dimension=0,
        tiled=True,
    ).astype(jnp.float32)
    own_rows = lax.dynamic_slice_in_dim(residual, lax.axis_index("tp") * quarter, quarter, 0)
    rows_mid = (own_rows.astype(jnp.float32) + mixed).astype(jnp.bfloat16)
    own_normed = row_norm(rows_mid.astype(jnp.float32), mlp_gain).astype(jnp.bfloat16)
    normed = lax.all_gather(own_normed, "tp", axis=0, tiled=True)
    gate = jnp.dot(
        normed,
        lax.all_gather(gate_weight, "sp", axis=0, tiled=True),
        preferred_element_type=jnp.float32,
    )
    upvals = jnp.dot(
        normed,
        lax.all_gather(up_weight, "sp", axis=0, tiled=True),
        preferred_element_type=jnp.float32,
    )
    full_down = lax.all_gather(down_weight, "sp", axis=1, tiled=True)
    hidden = (jax.nn.silu(gate) * upvals).astype(jnp.bfloat16)
    picked = hidden
    ffn = lax.psum_scatter(
        jnp.dot(picked, full_down, preferred_element_type=jnp.float32).astype(jnp.bfloat16),
        "tp",
        scatter_dimension=0,
        tiled=True,
    ).astype(jnp.float32)
    return (rows_mid.astype(jnp.float32) + ffn).astype(jnp.bfloat16)


MESH = pl.DeviceIdType.MESH
XS = 2
CS = 2
F32 = jnp.float32
BF16 = jnp.bfloat16


def dot_nt(a, b):
    return lax.dot_general(a, b, (((1,), (1,)), ((), ())), preferred_element_type=F32)


def dot_nn(a, b):
    return lax.dot_general(a, b, (((1,), (0,)), ((), ())), preferred_element_type=F32)


def kernel(
    nz,
    nt,
    q_ref,
    k_ref,
    v_ref,
    g_ref,
    ld_ref,
    hg_ref,
    res_ref,
    mg_ref,
    ow_hbm,
    gw_hbm,
    uw_hbm,
    dw_hbm,
    out_ref,
    ow,
    raw,
    turned,
    w,
    qrot,
    inner,
    cumx,
    contrib,
    c_out,
    t_out,
    c_in,
    t_in,
    p_out,
    tt_out,
    p_in,
    tt_in,
    s_own,
    s_out,
    s_in,
    retained,
    mix_out,
    mix_in,
    acc,
    norm_own,
    normed,
    gated,
    hidden,
    keep,
    s1,
    r1,
    s2,
    r2,
    s3,
    r3,
    ow_sem,
    raw_sem,
    own_sem,
    w_send,
    w_recv,
    f_send,
    f_recv,
    cx_send,
    cx_recv,
    pz_send,
    pz_recv,
    sx_send,
    sx_recv,
    mix_send,
    mix_recv,
    nz_send,
    nz_recv,
    nt_send,
    nt_recv,
    t1_send,
    t1_recv,
    t2_send,
    t2_recv,
    t3_send,
    t3_recv,
):
    sp = lax.axis_index("sp")
    tp = lax.axis_index("tp")
    z, x = sp // XS, lax.rem(sp, XS)
    y, c = tp // CS, lax.rem(tp, CS)
    rows = q_ref.shape[0]
    heads = ld_ref.shape[0]
    hh = heads // XS
    hd = q_ref.shape[1] // heads
    quarter = rows // nt
    share, width = w.shape[2], w.shape[3]
    group = XS * width
    x_peer = (z * XS + (1 - x), tp)
    c_peer = (sp, y * CS + (1 - c))
    y_peer = (sp, (1 - y) * CS + c)

    def z_at(d):
        return lax.rem(z + d, nz)

    def z_from(d):
        return lax.rem(z - d + nz, nz)

    def z_peer(d):
        return (z_at(d) * XS + x, tp)

    def t_at(d):
        return lax.rem(tp + d, nt)

    def t_peer(d):
        return (sp, t_at(d))

    def remote(src, dst, send, recv, peer):
        return pltpu.make_async_remote_copy(
            src_ref=src,
            dst_ref=dst,
            send_sem=send,
            recv_sem=recv,
            device_id=peer,
            device_id_type=MESH,
        )

    started = []

    def go(copy):
        copy.start()
        started.append(copy)
        return copy

    def piece(m, zz):
        at = pl.ds(pl.multiple_of(zz * share, 16), share)
        return dw_hbm.at[at] if m == 2 else turned.at[m, at]

    raw_copies = []
    for m, source in enumerate((gw_hbm, uw_hbm)):
        raw_copy = pltpu.make_async_copy(source, raw.at[m], raw_sem.at[m])
        raw_copy.start()
        raw_copies.append(raw_copy)
    ow_copy = pltpu.make_async_copy(ow_hbm, ow, ow_sem)
    own_copies = {}

    def take_own(m):
        own_copies[m] = pltpu.make_async_copy(piece(m, z), w.at[m, sp], own_sem.at[m])
        own_copies[m].start()

    take_own(2)
    ow_copy.start()

    barrier = pltpu.get_barrier_semaphore()
    peers = [z_peer(d) for d in range(1, nz)] + [x_peer] + [t_peer(d) for d in range(1, nt)]
    for peer in peers:
        pl.semaphore_signal(barrier, inc=1, device_id=peer, device_id_type=MESH)
    pl.semaphore_wait(barrier, len(peers))

    w_copies = {}

    def send_weight(m, d):
        w_copies[m, d] = go(
            remote(piece(m, z_at(d)), w.at[m, sp], w_send.at[m, d], w_recv.at[m, d], z_peer(d))
        )

    f_copies = {}

    def forward(m, d):
        slot = z_from(d) * XS + x
        if d == 0:
            own_copies[m].wait()
        else:
            w_copies[m, d].wait_recv()
        f_copies[m, d] = go(
            remote(w.at[m, slot], w.at[m, slot], f_send.at[m, d], f_recv.at[m, d], x_peer)
        )

    far = 2
    near = [d for d in range(1, nz) if d != far]
    send_weight(2, far)

    ti = lax.broadcasted_iota(jnp.int32, (rows, rows), 0)
    si = lax.broadcasted_iota(jnp.int32, (rows, rows), 1)
    lower = si <= ti
    cumul = lax.dot_general(
        ld_ref[...],
        (ti <= si).astype(F32),
        (((1,), (0,)), ((), ())),
        precision=lax.Precision.HIGHEST,
        preferred_element_type=F32,
    )
    half = hd // 2
    lane = lax.broadcasted_iota(jnp.int32, (1, hd), 1)
    low_half = lane < half
    index = jnp.where(low_half, lane, lane - half).astype(F32)
    freq = jnp.exp(index * (-math.log(10000.0) / (half - 1)))
    angles = (sp * rows + lax.broadcasted_iota(jnp.int32, (rows, hd), 0)).astype(F32) * freq
    cos = jnp.cos(angles)
    sin = jnp.sin(angles)
    sin = jnp.where(low_half, -sin, sin)
    for h in range(heads):
        cols = slice(h * hd, (h + 1) * hd)
        qf = q_ref[:, cols].astype(F32)
        kf = k_ref[:, cols].astype(F32)
        vb = v_ref[:, cols]
        qb = (qf * cos + pltpu.roll(qf, half, 1) * sin).astype(BF16)
        kb = ((kf * cos + pltpu.roll(kf, half, 1) * sin) * hd ** (-0.5)).astype(BF16)
        along = jnp.broadcast_to(cumul[h : h + 1, :], (rows, rows))
        cum = jnp.transpose(along)
        spread = cum - along
        weight = jnp.where(lower, jnp.exp(jnp.where(lower, spread, 0.0)), 0.0)
        probs = (dot_nt(qb, kb) * weight).astype(BF16)
        inner[:, cols] = dot_nn(probs, vb)
        last = cum[rows - 1 :, :]
        kw = kb.astype(F32) * jnp.exp(last - cum)
        cb = dot_nn(jnp.transpose(kw).astype(BF16), vb)
        contrib[h] = cb
        c_out[h] = cb.astype(BF16)
        t_out[h] = jnp.broadcast_to(jnp.exp(last), t_out.shape[1:])
        qrot[:, cols] = qb.astype(F32)
        cumx[:, cols] = jnp.exp(cum)
    mine_h, other_h = x * hh, (1 - x) * hh
    cx = go(remote(c_out.at[pl.ds(other_h, hh)], c_in, cx_send.at[0], cx_recv.at[0], x_peer))
    tx = go(remote(t_out, t_in, cx_send.at[1], cx_recv.at[1], x_peer))
    forward(2, 0)
    for m in range(2):
        raw_copies[m].wait()
        for j in range(raw.shape[2] // 128):
            turned[m, j * 128 : (j + 1) * 128, :] = jnp.transpose(
                raw[m, :, j * 128 : (j + 1) * 128]
            )
        take_own(m)
    cx.wait_recv()
    tx.wait_recv()
    first = x == 0
    for i in range(hh):
        own_c, own_t = contrib[mine_h + i], t_out[mine_h + i][:1]
        other_c, other_t = c_in[i].astype(F32), t_in[mine_h + i][:1]
        plane = jnp.where(first, other_t * own_c + other_c, own_t * other_c + own_c)
        p_out[i] = plane.astype(BF16)
        tt_out[i] = jnp.broadcast_to(own_t * other_t, tt_out.shape[1:])
    pz, tz = {}, {}
    for d in range(1, nz):
        pz[d] = go(remote(p_out, p_in.at[z], pz_send.at[0, d], pz_recv.at[0, d], z_peer(d)))
        tz[d] = go(remote(tt_out, tt_in.at[z], pz_send.at[1, d], pz_recv.at[1, d], z_peer(d)))
    for d in range(1, nz):
        pz[d].wait_recv()
        tz[d].wait_recv()
    send_weight(0, far)
    send_weight(0, near[0])
    p_in[z] = p_out[...]
    tt_in[z] = tt_out[...]
    for i in range(hh):
        state = jnp.zeros((hd, hd), F32)
        for zz in range(nz - 1):
            later = tt_in[zz, i][:1] * state + p_in[zz, i].astype(F32)
            state = jnp.where(zz < z, later, state)
        early_t = jnp.where(first, t_out[mine_h + i][:1], t_in[mine_h + i][:1])
        early_c = jnp.where(first, contrib[mine_h + i], c_in[i].astype(F32))
        after = early_t * state + early_c
        s_own[i] = jnp.where(first, state, after)
        s_out[i] = jnp.where(first, after, state).astype(BF16)
    sx = go(remote(s_out, s_in, sx_send, sx_recv, x_peer))
    forward(0, 0)
    forward(1, 0)
    forward(2, far)

    def finish(h, state, cols):
        cross = lax.dot_general(
            qrot[:, cols],
            state,
            (((1,), (0,)), ((), ())),
            precision=lax.Precision.HIGHEST,
            preferred_element_type=F32,
        )
        ret = inner[:, cols] + cumx[:, cols] * cross
        scale = lax.rsqrt(jnp.mean(ret * ret, axis=-1, keepdims=True) + EPS)
        gf = g_ref[:, cols].astype(F32)
        retained[:, cols] = (
            ret * scale * hg_ref[:, cols] * (gf / (1.0 + jnp.exp(-gf)))
        ).astype(BF16)

    sx.wait_recv()
    for h in range(heads):
        cols = slice(h * hd, (h + 1) * hd)
        i = h % hh
        mine = x == h // hh
        finish(h, jnp.where(mine, s_own[i], s_in[i].astype(F32)), cols)
    ow_copy.wait()
    mixes = []
    for d in list(range(1, nt)) + [0]:
        mine = pl.multiple_of(t_at(d) * quarter, quarter)
        part = dot_nn(retained[pl.ds(mine, quarter), :], ow[...]).astype(BF16)
        if d == 0:
            mix_in[tp] = part
        else:
            mix_out[d] = part
            mixes.append(
                go(
                    remote(
                        mix_out.at[d], mix_in.at[tp], mix_send.at[d], mix_recv.at[d], t_peer(d)
                    )
                )
            )
    for mix in mixes:
        mix.wait_recv()
    mixed = mix_in[0].astype(F32)
    for j in range(1, nt):
        mixed += mix_in[j].astype(F32)
    mine = pl.multiple_of(tp * quarter, quarter)
    mid = (res_ref[pl.ds(mine, quarter), :].astype(F32) + mixed).astype(BF16).astype(F32)
    for g in range(nz):
        acc[g] = mid[:, g * group : (g + 1) * group]
    norm_own[...] = (
        mid * lax.rsqrt(jnp.mean(mid * mid, axis=-1, keepdims=True) + EPS) * mg_ref[...]
    ).astype(BF16)
    normed[z, tp] = norm_own[...]
    tcopy = {}

    def share_rows(i, zz):
        rows_at = normed.at[zz, tp]
        for e, peer in ((1, c_peer), (2, y_peer)):
            tcopy[i, e] = go(
                remote(rows_at, rows_at, nt_send.at[i, e], nt_recv.at[i, e], peer)
            )

    def pass_rows(i, zz):
        rows_at = normed.at[zz, (1 - y) * CS + c]
        tcopy[i, 2].wait_recv()
        tcopy[i, 3] = go(remote(rows_at, rows_at, nt_send.at[i, 3], nt_recv.at[i, 3], c_peer))

    mate = z + 1 - 2 * lax.rem(z, 2)
    mate_peer = (mate * XS + x, tp)
    z_far, z_last = z_from(far), lax.rem(mate + far, nz)
    n_far = go(remote(norm_own, normed.at[z, tp], nz_send.at[0], nz_recv.at[0], z_peer(far)))
    n_mate = go(remote(norm_own, normed.at[z, tp], nz_send.at[1], nz_recv.at[1], mate_peer))
    share_rows(0, z)
    forward(0, far)
    n_far.wait_recv()
    far_rows = normed.at[z_far, tp]
    n_pass = go(remote(far_rows, far_rows, nz_send.at[2], nz_recv.at[2], mate_peer))
    share_rows(1, z_far)
    send_weight(0, near[1])
    send_weight(1, far)
    for m in (1, 2):
        for d in near:
            send_weight(m, d)
    forward(0, near[0])
    n_mate.wait_recv()
    share_rows(2, mate)
    pass_rows(0, z)
    pass_rows(1, z_far)
    n_pass.wait_recv()
    share_rows(3, z_last)
    pass_rows(2, mate)
    forward(0, near[1])
    pass_rows(3, z_last)
    forward(1, far)
    for d in range(nz):
        f_copies[0, d].wait_recv()
    for key in sorted(tcopy):
        if key[1] != 2:
            tcopy[key].wait_recv()

    ns = nz * XS

    def project(m, zz):
        block = normed[zz].reshape(rows, normed.shape[3])
        total = dot_nt(block[:, :width], w[m, 0])
        for s in range(1, ns):
            total += dot_nt(block[:, s * width : (s + 1) * width], w[m, s])
        return total

    def gate_rows(zz):
        gate = project(0, zz)
        gated[zz] = gate / (1.0 + jnp.exp(-gate))

    def up_rows(zz):
        hidden[zz * rows : (zz + 1) * rows, :] = (gated[zz] * project(1, zz)).astype(BF16)

    for zz in range(nz // 2):
        gate_rows(zz)
    forward(1, near[0])
    for zz in range(nz // 2, nz):
        gate_rows(zz)
    forward(1, near[1])
    for d in range(nz):
        f_copies[1, d].wait_recv()
    for zz in range(nz // 2):
        up_rows(zz)
    forward(2, near[0])
    for zz in range(nz // 2, nz):
        up_rows(zz)
    forward(2, near[1])

    t1, t2, t3 = {}, {}, {}
    low = c == 0

    def compute(b):
        f_copies[2, b].wait_recv()
        for u in range(XS):
            part = dot_nn(hidden[...], w[2, z_from(b) * XS + u])
            cols = slice(u * width, (u + 1) * width)
            for zz in range(nz):
                for yy in range(nt // CS):
                    at = zz * rows + yy * CS * quarter
                    even = part[at : at + quarter]
                    odd = part[at + quarter : at + 2 * quarter]
                    keep[b, yy, zz, :, cols] = jnp.where(low, even, odd)
                    s1[b, yy, zz, :, cols] = jnp.where(low, odd, even).astype(BF16)
        t1[b] = go(remote(s1.at[b], r1.at[b], t1_send.at[b], t1_recv.at[b], c_peer))

    def second(b):
        t1[b].wait_recv()
        s2[b] = (keep[b, 1 - y] + r1[b, 1 - y].astype(F32)).astype(BF16)
        t2[b] = go(remote(s2.at[b], r2.at[b], t2_send.at[b], t2_recv.at[b], y_peer))
        keep[b, y] = keep[b, y] + r1[b, y].astype(F32)

    def third(b):
        t2[b].wait_recv()
        for e in [far] + near:
            zz = z_at(e)
            s3[b, e] = (keep[b, y, zz] + r2[b, zz].astype(F32)).astype(BF16)
            t3[b, e] = go(
                remote(s3.at[b, e], r3.at[b, e], t3_send.at[b, e], t3_recv.at[b, e], z_peer(e))
            )
        g = z_from(b)
        acc[g] = acc[g] + keep[b, y, z] + r2[b, z].astype(F32)

    batches = [0, far] + near
    compute(0)
    compute(far)
    second(0)
    second(far)
    third(0)
    third(far)
    compute(near[0])
    second(near[0])
    compute(near[1])
    third(near[0])
    second(near[1])
    third(near[1])
    for b in batches:
        for e in [far] + near:
            t3[b, e].wait_recv()
            g = lax.rem(z - e - b + 2 * nz, nz)
            acc[g] = acc[g] + r3[b, e].astype(F32)
    for g in range(nz):
        out_ref[:, g * group : (g + 1) * group] = acc[g].astype(BF16)
    for copy in started:
        copy.wait_send()


def fast_body(
    queries,
    key_rows,
    value_rows,
    gate_input,
    log_decay,
    head_gain,
    out_weight,
    residual,
    mlp_gain,
    gate_weight,
    up_weight,
    down_weight,
):
    rows, wide = queries.shape
    heads = log_decay.shape[1]
    hd = wide // heads
    model = residual.shape[1]
    ns, nt = lax.axis_size("sp"), lax.axis_size("tp")
    nz = ns // XS
    quarter = rows // nt
    width, units = gate_weight.shape
    share = units // nz
    group = XS * width
    hh = heads // XS
    vmem = pl.BlockSpec(memory_space=pltpu.VMEM)
    anyspace = pl.BlockSpec(memory_space=pl.ANY)
    dma = pltpu.SemaphoreType.DMA
    scratch = [
        pltpu.VMEM(out_weight.shape, BF16),
        pltpu.VMEM((2, width, units), BF16),
        pltpu.VMEM((2, units, width), BF16),
        pltpu.VMEM((3, ns, share, width), BF16),
        pltpu.VMEM((rows, wide), F32),
        pltpu.VMEM((rows, wide), F32),
        pltpu.VMEM((rows, wide), F32),
        pltpu.VMEM((heads, hd, hd), F32),
        pltpu.VMEM((heads, hd, hd), BF16),
        pltpu.VMEM((heads, 8, hd), F32),
        pltpu.VMEM((hh, hd, hd), BF16),
        pltpu.VMEM((heads, 8, hd), F32),
        pltpu.VMEM((hh, hd, hd), BF16),
        pltpu.VMEM((hh, 8, hd), F32),
        pltpu.VMEM((nz, hh, hd, hd), BF16),
        pltpu.VMEM((nz, hh, 8, hd), F32),
        pltpu.VMEM((hh, hd, hd), F32),
        pltpu.VMEM((hh, hd, hd), BF16),
        pltpu.VMEM((hh, hd, hd), BF16),
        pltpu.VMEM((rows, wide), BF16),
        pltpu.VMEM((nt, quarter, model), BF16),
        pltpu.VMEM((nt, quarter, model), BF16),
        pltpu.VMEM((nz, quarter, group), F32),
        pltpu.VMEM((quarter, model), BF16),
        pltpu.VMEM((nz, nt, quarter, model), BF16),
        pltpu.VMEM((nz, rows, share), F32),
        pltpu.VMEM((nz * rows, share), BF16),
        pltpu.VMEM((nz, nt // CS, nz, quarter, group), F32),
        pltpu.VMEM((nz, nt // CS, nz, quarter, group), BF16),
        pltpu.VMEM((nz, nt // CS, nz, quarter, group), BF16),
        pltpu.VMEM((nz, nz, quarter, group), BF16),
        pltpu.VMEM((nz, nz, quarter, group), BF16),
        pltpu.VMEM((nz, nz, quarter, group), BF16),
        pltpu.VMEM((nz, nz, quarter, group), BF16),
        dma,
        dma((2,)),
        dma((3,)),
        dma((3, nz)),
        dma((3, nz)),
        dma((3, nz)),
        dma((3, nz)),
        dma((2,)),
        dma((2,)),
        dma((2, nz)),
        dma((2, nz)),
        dma,
        dma,
        dma((nt,)),
        dma((nt,)),
        dma((nz,)),
        dma((nz,)),
        dma((nz, nt)),
        dma((nz, nt)),
        dma((nz,)),
        dma((nz,)),
        dma((nz,)),
        dma((nz,)),
        dma((nz, nz)),
        dma((nz, nz)),
    ]
    return pl.pallas_call(
        functools.partial(kernel, nz, nt),
        out_shape=jax.ShapeDtypeStruct((quarter, model), BF16),
        in_specs=[vmem] * 8 + [anyspace] * 4,
        out_specs=vmem,
        scratch_shapes=scratch,
        compiler_params=pltpu.CompilerParams(
            collective_id=0, has_side_effects=True, vmem_limit_bytes=60 * 1024 * 1024
        ),
    )(
        queries,
        key_rows,
        value_rows,
        gate_input,
        log_decay.T,
        head_gain.reshape(1, wide),
        residual,
        mlp_gain.reshape(1, model),
        out_weight,
        gate_weight,
        up_weight,
        down_weight,
    )


def fits(mesh, queries, log_decay, gate_weight):
    ns, nt = mesh.shape["sp"], mesh.shape["tp"]
    tokens, wide = queries.shape
    if ns % XS or ns // XS != 4 or nt != 2 * CS or tokens // ns != BLOCK:
        return False
    nz = ns // XS
    hidden = gate_weight.shape[1] // nt
    return (
        gate_weight.shape[0] // ns % 128 == 0
        and hidden % (16 * nz) == 0
        and wide // log_decay.shape[1] == 128
        and BLOCK % (16 * nt) == 0
        and hidden % 128 == 0
        and log_decay.shape[1] // nt % XS == 0
    )


def solution(mesh):
    def run(*args):
        good = fits(mesh, args[0], args[4], args[9])
        return jax.shard_map(
            fast_body if good else body,
            mesh=mesh,
            in_specs=(
                P("sp", "tp"),
                P("sp", "tp"),
                P("sp", "tp"),
                P("sp", "tp"),
                P("sp", "tp"),
                P("tp"),
                P("tp", None),
                P("sp", None),
                P(),
                P("sp", "tp"),
                P("sp", "tp"),
                P("tp", "sp"),
            ),
            out_specs=P(("sp", "tp"), None),
            check_vma=False,
        )(*args)

    return run
```

```python
import functools
import math

import jax
import jax.numpy as jnp
from jax import lax
from jax.experimental import pallas as pl
from jax.experimental.pallas import tpu as pltpu
from jax.sharding import PartitionSpec as P

BLOCK = 128


EPS = 1e-06


def prefix_2(x, axis, join, neutral):
    place = lax.axis_index(axis)
    gathered = jax.tree.map(
        lambda a, kind: lax.all_gather(a.astype(kind), axis), x, (jnp.bfloat16, jnp.bfloat16)
    )
    state = jax.tree.map(lambda a, e: jnp.zeros_like(a) + jnp.asarray(e, a.dtype), x, neutral)

    def one(step, state):
        return join(
            state,
            jax.tree.map(
                lambda a, own: lax.dynamic_index_in_dim(a, step, 0, False).astype(own.dtype),
                gathered,
                x,
            ),
        )

    return lax.fori_loop(0, place, one, state)


def rotate(values_in, positions):
    half = values_in.shape[-1] // 2
    freq = 10000.0 ** (-jnp.linspace(0.0, 1.0, half, dtype=jnp.float32))
    angles = positions * freq
    angles = jnp.concatenate([angles, angles], axis=-1)
    first = values_in[..., :half]
    second = values_in[..., half:]
    turned = jnp.concatenate([-second, first], axis=-1)
    return values_in * jnp.cos(angles) + turned * jnp.sin(angles)


def row_norm(stream, gain):
    return stream * lax.rsqrt(jnp.mean(stream * stream, axis=-1, keepdims=True) + EPS) * gain


def join_states(earlier, later):
    return (earlier[0] * later[0], later[0][:, None, None] * earlier[1] + later[1])


def body(
    queries,
    key_rows,
    value_rows,
    gate_input,
    log_decay,
    head_gain,
    out_weight,
    residual,
    mlp_gain,
    gate_weight,
    up_weight,
    down_weight,
):
    tok_rows = queries.shape[0]
    heads_here = log_decay.shape[1]
    head_size = head_gain.shape[0] // heads_here
    quarter = tok_rows // lax.axis_size("tp")
    offset = lax.axis_index("sp") * tok_rows
    positions = (offset + lax.iota(jnp.int32, tok_rows)).astype(jnp.float32)[:, None, None]
    q_rot = rotate(
        queries.reshape(tok_rows, heads_here, head_size).astype(jnp.float32), positions
    ).astype(jnp.bfloat16)
    k_rot = (
        rotate(key_rows.reshape(tok_rows, heads_here, head_size).astype(jnp.float32), positions)
        * head_size ** (-0.5)
    ).astype(jnp.bfloat16)
    blocks = tok_rows // BLOCK
    q_blocks = q_rot.reshape(blocks, BLOCK, heads_here, head_size)
    k_blocks = k_rot.reshape(blocks, BLOCK, heads_here, head_size)
    v_blocks = value_rows.reshape(blocks, BLOCK, heads_here, head_size)
    cumul = jnp.cumsum(log_decay.reshape(blocks, BLOCK, heads_here), axis=1)
    by_head = cumul.transpose(0, 2, 1)
    lower = jnp.tril(jnp.ones((BLOCK, BLOCK), dtype=bool))
    spread = by_head[:, :, :, None] - by_head[:, :, None, :]
    weight = jnp.where(lower, jnp.exp(jnp.where(lower, spread, 0.0)), 0.0)
    scores = jnp.einsum("nthd,nshd->nhts", q_blocks, k_blocks, preferred_element_type=jnp.float32)
    probs = (scores * weight).astype(jnp.bfloat16)
    inner = jnp.einsum("nhts,nshe->nthe", probs, v_blocks, preferred_element_type=jnp.float32)
    k_weighted = (
        k_blocks.astype(jnp.float32) * jnp.exp(cumul[:, -1:, :] - cumul)[..., None]
    ).astype(jnp.bfloat16)
    contrib = jnp.einsum(
        "nshd,nshe->nhde", k_weighted, v_blocks, preferred_element_type=jnp.float32
    )
    totals = jnp.exp(cumul[:, -1, :])

    def advance(carry, items):
        state, prefix = carry
        factor, update = items
        return ((state * factor[:, None, None] + update, prefix * factor), (state, prefix))

    start_state = jnp.zeros((heads_here, head_size, head_size), jnp.float32)
    start_prefix = jnp.ones((heads_here,), jnp.float32)
    (dev_state, dev_total), (local_before, prefixes) = lax.scan(
        advance, (start_state, start_prefix), (totals, contrib)
    )
    _, incoming = prefix_2((dev_total, dev_state), "sp", join_states, (start_prefix, start_state))
    before = local_before + prefixes[:, :, None, None] * incoming[None]
    cross = jnp.einsum(
        "nthd,nhde->nthe", q_blocks.astype(jnp.float32), before, precision=lax.Precision.HIGHEST
    )
    cross = cross * jnp.exp(cumul)[..., None]
    result = (inner + cross).reshape(tok_rows, heads_here, head_size)
    result = row_norm(result, head_gain.reshape(heads_here, head_size)).reshape(
        tok_rows, heads_here * head_size
    )
    retained = (result * jax.nn.silu(gate_input.astype(jnp.float32))).astype(jnp.bfloat16)
    picked = retained
    mixed = lax.psum_scatter(
        jnp.dot(picked, out_weight, preferred_element_type=jnp.float32).astype(jnp.bfloat16),
        "tp",
        scatter_dimension=0,
        tiled=True,
    ).astype(jnp.float32)
    own_rows = lax.dynamic_slice_in_dim(residual, lax.axis_index("tp") * quarter, quarter, 0)
    rows_mid = (own_rows.astype(jnp.float32) + mixed).astype(jnp.bfloat16)
    own_normed = row_norm(rows_mid.astype(jnp.float32), mlp_gain).astype(jnp.bfloat16)
    normed = lax.all_gather(own_normed, "tp", axis=0, tiled=True)
    gate = jnp.dot(
        normed,
        lax.all_gather(gate_weight, "sp", axis=0, tiled=True),
        preferred_element_type=jnp.float32,
    )
    upvals = jnp.dot(
        normed,
        lax.all_gather(up_weight, "sp", axis=0, tiled=True),
        preferred_element_type=jnp.float32,
    )
    full_down = lax.all_gather(down_weight, "sp", axis=1, tiled=True)
    hidden = (jax.nn.silu(gate) * upvals).astype(jnp.bfloat16)
    picked = hidden
    ffn = lax.psum_scatter(
        jnp.dot(picked, full_down, preferred_element_type=jnp.float32).astype(jnp.bfloat16),
        "tp",
        scatter_dimension=0,
        tiled=True,
    ).astype(jnp.float32)
    return (rows_mid.astype(jnp.float32) + ffn).astype(jnp.bfloat16)


MESH = pl.DeviceIdType.MESH
XS = 2
CS = 2
F32 = jnp.float32
BF16 = jnp.bfloat16


def dot_nt(a, b):
    return lax.dot_general(a, b, (((1,), (1,)), ((), ())), preferred_element_type=F32)


def dot_nn(a, b):
    return lax.dot_general(a, b, (((1,), (0,)), ((), ())), preferred_element_type=F32)


def kernel(
    nz,
    nt,
    q_ref,
    k_ref,
    v_ref,
    g_ref,
    ld_ref,
    hg_ref,
    res_ref,
    mg_ref,
    ow_hbm,
    gw_hbm,
    uw_hbm,
    dw_hbm,
    out_ref,
    ow,
    raw,
    turned,
    w,
    qrot,
    inner,
    cumx,
    contrib,
    c_out,
    t_out,
    c_in,
    t_in,
    p_out,
    tt_out,
    p_in,
    tt_in,
    s_own,
    s_out,
    s_in,
    retained,
    mix_out,
    mix_in,
    acc,
    norm_own,
    normed,
    gated,
    hidden,
    keep,
    s1,
    r1,
    s2,
    r2,
    s3,
    r3,
    ow_sem,
    raw_sem,
    own_sem,
    w_send,
    w_recv,
    f_send,
    f_recv,
    cx_send,
    cx_recv,
    pz_send,
    pz_recv,
    sx_send,
    sx_recv,
    mix_send,
    mix_recv,
    nz_send,
    nz_recv,
    nt_send,
    nt_recv,
    t1_send,
    t1_recv,
    t2_send,
    t2_recv,
    t3_send,
    t3_recv,
):
    sp = lax.axis_index("sp")
    tp = lax.axis_index("tp")
    z, x = sp // XS, lax.rem(sp, XS)
    y, c = tp // CS, lax.rem(tp, CS)
    rows = q_ref.shape[0]
    heads = ld_ref.shape[0]
    hh = heads // XS
    hd = q_ref.shape[1] // heads
    quarter = rows // nt
    share, width = w.shape[2], w.shape[3]
    group = XS * width
    x_peer = (z * XS + (1 - x), tp)
    c_peer = (sp, y * CS + (1 - c))
    y_peer = (sp, (1 - y) * CS + c)

    def z_at(d):
        return lax.rem(z + d, nz)

    def z_from(d):
        return lax.rem(z - d + nz, nz)

    def z_peer(d):
        return (z_at(d) * XS + x, tp)

    def t_at(d):
        return lax.rem(tp + d, nt)

    def t_peer(d):
        return (sp, t_at(d))

    def remote(src, dst, send, recv, peer):
        return pltpu.make_async_remote_copy(
            src_ref=src,
            dst_ref=dst,
            send_sem=send,
            recv_sem=recv,
            device_id=peer,
            device_id_type=MESH,
        )

    started = []

    def go(copy):
        copy.start()
        started.append(copy)
        return copy

    def piece(m, zz):
        at = pl.ds(pl.multiple_of(zz * share, 16), share)
        return dw_hbm.at[at] if m == 2 else turned.at[m, at]

    raw_copies = []
    for m, source in enumerate((gw_hbm, uw_hbm)):
        raw_copy = pltpu.make_async_copy(source, raw.at[m], raw_sem.at[m])
        raw_copy.start()
        raw_copies.append(raw_copy)
    ow_copy = pltpu.make_async_copy(ow_hbm, ow, ow_sem)
    own_copies = {}

    def take_own(m):
        own_copies[m] = pltpu.make_async_copy(piece(m, z), w.at[m, sp], own_sem.at[m])
        own_copies[m].start()

    take_own(2)
    ow_copy.start()

    barrier = pltpu.get_barrier_semaphore()
    peers = [z_peer(d) for d in range(1, nz)] + [x_peer] + [t_peer(d) for d in range(1, nt)]
    for peer in peers:
        pl.semaphore_signal(barrier, inc=1, device_id=peer, device_id_type=MESH)
    for m in range(2):
        raw_copies[m].wait()
        for j in range(raw.shape[2] // 128):
            turned[m, j * 128 : (j + 1) * 128, :] = jnp.transpose(
                raw[m, :, j * 128 : (j + 1) * 128]
            )
        take_own(m)
    pl.semaphore_wait(barrier, len(peers))

    w_copies = {}

    def send_weight(m, d):
        w_copies[m, d] = go(
            remote(piece(m, z_at(d)), w.at[m, sp], w_send.at[m, d], w_recv.at[m, d], z_peer(d))
        )

    f_copies = {}

    def forward(m, d):
        slot = z_from(d) * XS + x
        if d == 0:
            own_copies[m].wait()
        else:
            w_copies[m, d].wait_recv()
        f_copies[m, d] = go(
            remote(w.at[m, slot], w.at[m, slot], f_send.at[m, d], f_recv.at[m, d], x_peer)
        )

    far = 2
    near = [d for d in range(1, nz) if d != far]
    send_weight(1, far)

    ti = lax.broadcasted_iota(jnp.int32, (rows, rows), 0)
    si = lax.broadcasted_iota(jnp.int32, (rows, rows), 1)
    lower = si <= ti
    cumul = lax.dot_general(
        ld_ref[...],
        (ti <= si).astype(F32),
        (((1,), (0,)), ((), ())),
        precision=lax.Precision.HIGHEST,
        preferred_element_type=F32,
    )
    half = hd // 2
    lane = lax.broadcasted_iota(jnp.int32, (1, hd), 1)
    low_half = lane < half
    index = jnp.where(low_half, lane, lane - half).astype(F32)
    freq = jnp.exp(index * (-math.log(10000.0) / (half - 1)))
    angles = (sp * rows + lax.broadcasted_iota(jnp.int32, (rows, hd), 0)).astype(F32) * freq
    cos = jnp.cos(angles)
    sin = jnp.sin(angles)
    sin = jnp.where(low_half, -sin, sin)
    for h in range(heads):
        cols = slice(h * hd, (h + 1) * hd)
        qf = q_ref[:, cols].astype(F32)
        kf = k_ref[:, cols].astype(F32)
        vb = v_ref[:, cols]
        qb = (qf * cos + pltpu.roll(qf, half, 1) * sin).astype(BF16)
        kb = ((kf * cos + pltpu.roll(kf, half, 1) * sin) * hd ** (-0.5)).astype(BF16)
        along = jnp.broadcast_to(cumul[h : h + 1, :], (rows, rows))
        cum = jnp.transpose(along)
        spread = cum - along
        weight = jnp.where(lower, jnp.exp(jnp.where(lower, spread, 0.0)), 0.0)
        probs = (dot_nt(qb, kb) * weight).astype(BF16)
        inner[:, cols] = dot_nn(probs, vb)
        last = cum[rows - 1 :, :]
        kw = kb.astype(F32) * jnp.exp(last - cum)
        cb = dot_nn(jnp.transpose(kw).astype(BF16), vb)
        contrib[h] = cb
        c_out[h] = cb.astype(BF16)
        t_out[h] = jnp.broadcast_to(jnp.exp(last), t_out.shape[1:])
        qrot[:, cols] = qb.astype(F32)
        cumx[:, cols] = jnp.exp(cum)
    mine_h, other_h = x * hh, (1 - x) * hh
    cx = go(remote(c_out.at[pl.ds(other_h, hh)], c_in, cx_send.at[0], cx_recv.at[0], x_peer))
    tx = go(remote(t_out, t_in, cx_send.at[1], cx_recv.at[1], x_peer))
    forward(1, 0)
    cx.wait_recv()
    tx.wait_recv()
    first = x == 0
    for i in range(hh):
        own_c, own_t = contrib[mine_h + i], t_out[mine_h + i][:1]
        other_c, other_t = c_in[i].astype(F32), t_in[mine_h + i][:1]
        plane = jnp.where(first, other_t * own_c + other_c, own_t * other_c + own_c)
        p_out[i] = plane.astype(BF16)
        tt_out[i] = jnp.broadcast_to(own_t * other_t, tt_out.shape[1:])
    pz, tz = {}, {}
    for d in range(1, nz):
        pz[d] = go(remote(p_out, p_in.at[z], pz_send.at[0, d], pz_recv.at[0, d], z_peer(d)))
        tz[d] = go(remote(tt_out, tt_in.at[z], pz_send.at[1, d], pz_recv.at[1, d], z_peer(d)))
    for d in range(1, nz):
        pz[d].wait_recv()
        tz[d].wait_recv()
    send_weight(0, far)
    send_weight(0, near[0])
    p_in[z] = p_out[...]
    tt_in[z] = tt_out[...]
    for i in range(hh):
        state = jnp.zeros((hd, hd), F32)
        for zz in range(nz - 1):
            later = tt_in[zz, i][:1] * state + p_in[zz, i].astype(F32)
            state = jnp.where(zz < z, later, state)
        early_t = jnp.where(first, t_out[mine_h + i][:1], t_in[mine_h + i][:1])
        early_c = jnp.where(first, contrib[mine_h + i], c_in[i].astype(F32))
        after = early_t * state + early_c
        s_own[i] = jnp.where(first, state, after)
        s_out[i] = jnp.where(first, after, state).astype(BF16)
    sx = go(remote(s_out, s_in, sx_send, sx_recv, x_peer))
    forward(0, 0)
    forward(1, far)

    def finish(h, state, cols):
        cross = lax.dot_general(
            qrot[:, cols],
            state,
            (((1,), (0,)), ((), ())),
            precision=lax.Precision.HIGHEST,
            preferred_element_type=F32,
        )
        ret = inner[:, cols] + cumx[:, cols] * cross
        scale = lax.rsqrt(jnp.mean(ret * ret, axis=-1, keepdims=True) + EPS)
        gf = g_ref[:, cols].astype(F32)
        retained[:, cols] = (
            ret * scale * hg_ref[:, cols] * (gf / (1.0 + jnp.exp(-gf)))
        ).astype(BF16)

    sx.wait_recv()
    for h in range(heads):
        cols = slice(h * hd, (h + 1) * hd)
        i = h % hh
        mine = x == h // hh
        finish(h, jnp.where(mine, s_own[i], s_in[i].astype(F32)), cols)
    ow_copy.wait()
    mixes = []
    for d in list(range(1, nt)) + [0]:
        mine = pl.multiple_of(t_at(d) * quarter, quarter)
        part = dot_nn(retained[pl.ds(mine, quarter), :], ow[...]).astype(BF16)
        if d == 0:
            mix_in[tp] = part
        else:
            mix_out[d] = part
            mixes.append(
                go(
                    remote(
                        mix_out.at[d], mix_in.at[tp], mix_send.at[d], mix_recv.at[d], t_peer(d)
                    )
                )
            )
    for mix in mixes:
        mix.wait_recv()
    mixed = mix_in[0].astype(F32)
    for j in range(1, nt):
        mixed += mix_in[j].astype(F32)
    mine = pl.multiple_of(tp * quarter, quarter)
    mid = (res_ref[pl.ds(mine, quarter), :].astype(F32) + mixed).astype(BF16).astype(F32)
    for g in range(nz):
        for u in range(XS):
            at = g * group + u * width
            acc[g, u] = mid[:, at : at + width]
    norm_own[...] = (
        mid * lax.rsqrt(jnp.mean(mid * mid, axis=-1, keepdims=True) + EPS) * mg_ref[...]
    ).astype(BF16)
    normed[z, tp] = norm_own[...]
    tcopy = {}

    def share_rows(i, zz):
        rows_at = normed.at[zz, tp]
        for e, peer in ((1, c_peer), (2, y_peer)):
            tcopy[i, e] = go(
                remote(rows_at, rows_at, nt_send.at[i, e], nt_recv.at[i, e], peer)
            )

    def pass_rows(i, zz):
        rows_at = normed.at[zz, (1 - y) * CS + c]
        tcopy[i, 2].wait_recv()
        tcopy[i, 3] = go(remote(rows_at, rows_at, nt_send.at[i, 3], nt_recv.at[i, 3], c_peer))

    mate = z + 1 - 2 * lax.rem(z, 2)
    mate_peer = (mate * XS + x, tp)
    z_far, z_last = z_from(far), lax.rem(mate + far, nz)
    n_far = go(remote(norm_own, normed.at[z, tp], nz_send.at[0], nz_recv.at[0], z_peer(far)))
    n_mate = go(remote(norm_own, normed.at[z, tp], nz_send.at[1], nz_recv.at[1], mate_peer))
    share_rows(0, z)
    forward(0, far)
    forward(2, 0)
    n_far.wait_recv()
    far_rows = normed.at[z_far, tp]
    n_pass = go(remote(far_rows, far_rows, nz_send.at[2], nz_recv.at[2], mate_peer))
    share_rows(1, z_far)
    send_weight(0, near[1])
    for d in near:
        send_weight(1, d)
    for d in [far] + near:
        send_weight(2, d)
    forward(0, near[0])
    n_mate.wait_recv()
    share_rows(2, mate)
    pass_rows(0, z)
    pass_rows(1, z_far)
    n_pass.wait_recv()
    share_rows(3, z_last)
    pass_rows(2, mate)
    forward(0, near[1])
    pass_rows(3, z_last)
    forward(1, near[0])
    for d in range(nz):
        f_copies[0, d].wait_recv()
    for key in sorted(tcopy):
        if key[1] != 2:
            tcopy[key].wait_recv()

    ns = nz * XS

    def project(m, zz):
        block = normed[zz].reshape(rows, normed.shape[3])
        total = dot_nt(block[:, :width], w[m, 0])
        for s in range(1, ns):
            total += dot_nt(block[:, s * width : (s + 1) * width], w[m, s])
        return total

    def gate_rows(zz):
        gate = project(0, zz)
        gated[zz] = gate / (1.0 + jnp.exp(-gate))

    def up_rows(zz):
        hidden[zz * rows : (zz + 1) * rows, :] = (gated[zz] * project(1, zz)).astype(BF16)

    for zz in range(nz // 2):
        gate_rows(zz)
    forward(1, near[1])
    for zz in range(nz // 2, nz):
        gate_rows(zz)
    forward(2, far)
    for d in range(nz):
        f_copies[1, d].wait_recv()
    for zz in range(nz):
        up_rows(zz)

    t1, t2, t3 = {}, {}, {}
    low = c == 0

    def side(u):
        return x if u == 0 else 1 - x

    def compute(b, u):
        if u:
            f_copies[2, b].wait_recv()
        part = dot_nn(hidden[...], w[2, z_from(b) * XS + side(u)])
        for zz in range(nz):
            for yy in range(nt // CS):
                at = zz * rows + yy * CS * quarter
                even = part[at : at + quarter]
                odd = part[at + quarter : at + 2 * quarter]
                keep[b, u, yy, zz] = jnp.where(low, even, odd)
                s1[b, u, yy, zz] = jnp.where(low, odd, even).astype(BF16)
        t1[b, u] = go(
            remote(s1.at[b, u], r1.at[b, u], t1_send.at[b, u], t1_recv.at[b, u], c_peer)
        )

    def second(b, u):
        t1[b, u].wait_recv()
        s2[b, u] = (keep[b, u, 1 - y] + r1[b, u, 1 - y].astype(F32)).astype(BF16)
        t2[b, u] = go(
            remote(s2.at[b, u], r2.at[b, u], t2_send.at[b, u], t2_recv.at[b, u], y_peer)
        )
        keep[b, u, y] = keep[b, u, y] + r1[b, u, y].astype(F32)

    def third(b, u):
        t2[b, u].wait_recv()
        for e in [far] + near:
            zz = z_at(e)
            s3[b, u, e] = (keep[b, u, y, zz] + r2[b, u, zz].astype(F32)).astype(BF16)
            t3[b, u, e] = go(
                remote(
                    s3.at[b, u, e],
                    r3.at[b, u, e],
                    t3_send.at[b, u, e],
                    t3_recv.at[b, u, e],
                    z_peer(e),
                )
            )
        g, v = z_from(b), side(u)
        acc[g, v] = acc[g, v] + keep[b, u, y, z] + r2[b, u, z].astype(F32)

    n0, n1 = near
    compute(0, 0)
    compute(0, 1)
    compute(far, 0)
    second(0, 0)
    second(0, 1)
    forward(2, n0)
    compute(n0, 0)
    compute(far, 1)
    second(far, 0)
    forward(2, n1)
    compute(n1, 0)
    second(n0, 0)
    second(far, 1)
    third(0, 0)
    third(0, 1)
    second(n1, 0)
    compute(n0, 1)
    third(far, 0)
    third(n0, 0)
    second(n0, 1)
    compute(n1, 1)
    third(far, 1)
    second(n1, 1)
    third(n1, 0)
    third(n0, 1)
    third(n1, 1)
    order = [(0, 0), (0, 1), (far, 0), (n0, 0), (far, 1), (n1, 0), (n0, 1), (n1, 1)]
    for b, u in order:
        for e in [far] + near:
            t3[b, u, e].wait_recv()
            g, v = lax.rem(z - e - b + 2 * nz, nz), side(u)
            acc[g, v] = acc[g, v] + r3[b, u, e].astype(F32)
    for g in range(nz):
        for u in range(XS):
            at = g * group + u * width
            out_ref[:, at : at + width] = acc[g, u].astype(BF16)
    for copy in started:
        copy.wait_send()


def fast_body(
    queries,
    key_rows,
    value_rows,
    gate_input,
    log_decay,
    head_gain,
    out_weight,
    residual,
    mlp_gain,
    gate_weight,
    up_weight,
    down_weight,
):
    rows, wide = queries.shape
    heads = log_decay.shape[1]
    hd = wide // heads
    model = residual.shape[1]
    ns, nt = lax.axis_size("sp"), lax.axis_size("tp")
    nz = ns // XS
    quarter = rows // nt
    width, units = gate_weight.shape
    share = units // nz
    group = XS * width
    hh = heads // XS
    vmem = pl.BlockSpec(memory_space=pltpu.VMEM)
    anyspace = pl.BlockSpec(memory_space=pl.ANY)
    dma = pltpu.SemaphoreType.DMA
    scratch = [
        pltpu.VMEM(out_weight.shape, BF16),
        pltpu.VMEM((2, width, units), BF16),
        pltpu.VMEM((2, units, width), BF16),
        pltpu.VMEM((3, ns, share, width), BF16),
        pltpu.VMEM((rows, wide), F32),
        pltpu.VMEM((rows, wide), F32),
        pltpu.VMEM((rows, wide), F32),
        pltpu.VMEM((heads, hd, hd), F32),
        pltpu.VMEM((heads, hd, hd), BF16),
        pltpu.VMEM((heads, 8, hd), F32),
        pltpu.VMEM((hh, hd, hd), BF16),
        pltpu.VMEM((heads, 8, hd), F32),
        pltpu.VMEM((hh, hd, hd), BF16),
        pltpu.VMEM((hh, 8, hd), F32),
        pltpu.VMEM((nz, hh, hd, hd), BF16),
        pltpu.VMEM((nz, hh, 8, hd), F32),
        pltpu.VMEM((hh, hd, hd), F32),
        pltpu.VMEM((hh, hd, hd), BF16),
        pltpu.VMEM((hh, hd, hd), BF16),
        pltpu.VMEM((rows, wide), BF16),
        pltpu.VMEM((nt, quarter, model), BF16),
        pltpu.VMEM((nt, quarter, model), BF16),
        pltpu.VMEM((nz, XS, quarter, width), F32),
        pltpu.VMEM((quarter, model), BF16),
        pltpu.VMEM((nz, nt, quarter, model), BF16),
        pltpu.VMEM((nz, rows, share), F32),
        pltpu.VMEM((nz * rows, share), BF16),
        pltpu.VMEM((nz, XS, nt // CS, nz, quarter, width), F32),
        pltpu.VMEM((nz, XS, nt // CS, nz, quarter, width), BF16),
        pltpu.VMEM((nz, XS, nt // CS, nz, quarter, width), BF16),
        pltpu.VMEM((nz, XS, nz, quarter, width), BF16),
        pltpu.VMEM((nz, XS, nz, quarter, width), BF16),
        pltpu.VMEM((nz, XS, nz, quarter, width), BF16),
        pltpu.VMEM((nz, XS, nz, quarter, width), BF16),
        dma,
        dma((2,)),
        dma((3,)),
        dma((3, nz)),
        dma((3, nz)),
        dma((3, nz)),
        dma((3, nz)),
        dma((2,)),
        dma((2,)),
        dma((2, nz)),
        dma((2, nz)),
        dma,
        dma,
        dma((nt,)),
        dma((nt,)),
        dma((nz,)),
        dma((nz,)),
        dma((nz, nt)),
        dma((nz, nt)),
        dma((nz, XS)),
        dma((nz, XS)),
        dma((nz, XS)),
        dma((nz, XS)),
        dma((nz, XS, nz)),
        dma((nz, XS, nz)),
    ]
    return pl.pallas_call(
        functools.partial(kernel, nz, nt),
        out_shape=jax.ShapeDtypeStruct((quarter, model), BF16),
        in_specs=[vmem] * 8 + [anyspace] * 4,
        out_specs=vmem,
        scratch_shapes=scratch,
        compiler_params=pltpu.CompilerParams(
            collective_id=0, has_side_effects=True, vmem_limit_bytes=60 * 1024 * 1024
        ),
    )(
        queries,
        key_rows,
        value_rows,
        gate_input,
        log_decay.T,
        head_gain.reshape(1, wide),
        residual,
        mlp_gain.reshape(1, model),
        out_weight,
        gate_weight,
        up_weight,
        down_weight,
    )


def fits(mesh, queries, log_decay, gate_weight):
    ns, nt = mesh.shape["sp"], mesh.shape["tp"]
    tokens, wide = queries.shape
    if ns % XS or ns // XS != 4 or nt != 2 * CS or tokens // ns != BLOCK:
        return False
    nz = ns // XS
    hidden = gate_weight.shape[1] // nt
    return (
        gate_weight.shape[0] // ns % 128 == 0
        and hidden % (16 * nz) == 0
        and wide // log_decay.shape[1] == 128
        and BLOCK % (16 * nt) == 0
        and hidden % 128 == 0
        and log_decay.shape[1] // nt % XS == 0
    )


def solution(mesh):
    def run(*args):
        good = fits(mesh, args[0], args[4], args[9])
        return jax.shard_map(
            fast_body if good else body,
            mesh=mesh,
            in_specs=(
                P("sp", "tp"),
                P("sp", "tp"),
                P("sp", "tp"),
                P("sp", "tp"),
                P("sp", "tp"),
                P("tp"),
                P("tp", None),
                P("sp", None),
                P(),
                P("sp", "tp"),
                P("sp", "tp"),
                P("tp", "sp"),
            ),
            out_specs=P(("sp", "tp"), None),
            check_vma=False,
        )(*args)

    return run
```

```python
import functools
import math

import jax
import jax.numpy as jnp
from jax import lax
from jax.experimental import pallas as pl
from jax.experimental.pallas import tpu as pltpu
from jax.sharding import PartitionSpec as P

BLOCK = 128


EPS = 1e-06


def prefix_2(x, axis, join, neutral):
    place = lax.axis_index(axis)
    gathered = jax.tree.map(
        lambda a, kind: lax.all_gather(a.astype(kind), axis), x, (jnp.bfloat16, jnp.bfloat16)
    )
    state = jax.tree.map(lambda a, e: jnp.zeros_like(a) + jnp.asarray(e, a.dtype), x, neutral)

    def one(step, state):
        return join(
            state,
            jax.tree.map(
                lambda a, own: lax.dynamic_index_in_dim(a, step, 0, False).astype(own.dtype),
                gathered,
                x,
            ),
        )

    return lax.fori_loop(0, place, one, state)


def rotate(values_in, positions):
    half = values_in.shape[-1] // 2
    freq = 10000.0 ** (-jnp.linspace(0.0, 1.0, half, dtype=jnp.float32))
    angles = positions * freq
    angles = jnp.concatenate([angles, angles], axis=-1)
    first = values_in[..., :half]
    second = values_in[..., half:]
    turned = jnp.concatenate([-second, first], axis=-1)
    return values_in * jnp.cos(angles) + turned * jnp.sin(angles)


def row_norm(stream, gain):
    return stream * lax.rsqrt(jnp.mean(stream * stream, axis=-1, keepdims=True) + EPS) * gain


def join_states(earlier, later):
    return (earlier[0] * later[0], later[0][:, None, None] * earlier[1] + later[1])


def body(
    queries,
    key_rows,
    value_rows,
    gate_input,
    log_decay,
    head_gain,
    out_weight,
    residual,
    mlp_gain,
    gate_weight,
    up_weight,
    down_weight,
):
    tok_rows = queries.shape[0]
    heads_here = log_decay.shape[1]
    head_size = head_gain.shape[0] // heads_here
    quarter = tok_rows // lax.axis_size("tp")
    offset = lax.axis_index("sp") * tok_rows
    positions = (offset + lax.iota(jnp.int32, tok_rows)).astype(jnp.float32)[:, None, None]
    q_rot = rotate(
        queries.reshape(tok_rows, heads_here, head_size).astype(jnp.float32), positions
    ).astype(jnp.bfloat16)
    k_rot = (
        rotate(key_rows.reshape(tok_rows, heads_here, head_size).astype(jnp.float32), positions)
        * head_size ** (-0.5)
    ).astype(jnp.bfloat16)
    blocks = tok_rows // BLOCK
    q_blocks = q_rot.reshape(blocks, BLOCK, heads_here, head_size)
    k_blocks = k_rot.reshape(blocks, BLOCK, heads_here, head_size)
    v_blocks = value_rows.reshape(blocks, BLOCK, heads_here, head_size)
    cumul = jnp.cumsum(log_decay.reshape(blocks, BLOCK, heads_here), axis=1)
    by_head = cumul.transpose(0, 2, 1)
    lower = jnp.tril(jnp.ones((BLOCK, BLOCK), dtype=bool))
    spread = by_head[:, :, :, None] - by_head[:, :, None, :]
    weight = jnp.where(lower, jnp.exp(jnp.where(lower, spread, 0.0)), 0.0)
    scores = jnp.einsum("nthd,nshd->nhts", q_blocks, k_blocks, preferred_element_type=jnp.float32)
    probs = (scores * weight).astype(jnp.bfloat16)
    inner = jnp.einsum("nhts,nshe->nthe", probs, v_blocks, preferred_element_type=jnp.float32)
    k_weighted = (
        k_blocks.astype(jnp.float32) * jnp.exp(cumul[:, -1:, :] - cumul)[..., None]
    ).astype(jnp.bfloat16)
    contrib = jnp.einsum(
        "nshd,nshe->nhde", k_weighted, v_blocks, preferred_element_type=jnp.float32
    )
    totals = jnp.exp(cumul[:, -1, :])

    def advance(carry, items):
        state, prefix = carry
        factor, update = items
        return ((state * factor[:, None, None] + update, prefix * factor), (state, prefix))

    start_state = jnp.zeros((heads_here, head_size, head_size), jnp.float32)
    start_prefix = jnp.ones((heads_here,), jnp.float32)
    (dev_state, dev_total), (local_before, prefixes) = lax.scan(
        advance, (start_state, start_prefix), (totals, contrib)
    )
    _, incoming = prefix_2((dev_total, dev_state), "sp", join_states, (start_prefix, start_state))
    before = local_before + prefixes[:, :, None, None] * incoming[None]
    cross = jnp.einsum(
        "nthd,nhde->nthe", q_blocks.astype(jnp.float32), before, precision=lax.Precision.HIGHEST
    )
    cross = cross * jnp.exp(cumul)[..., None]
    result = (inner + cross).reshape(tok_rows, heads_here, head_size)
    result = row_norm(result, head_gain.reshape(heads_here, head_size)).reshape(
        tok_rows, heads_here * head_size
    )
    retained = (result * jax.nn.silu(gate_input.astype(jnp.float32))).astype(jnp.bfloat16)
    picked = retained
    mixed = lax.psum_scatter(
        jnp.dot(picked, out_weight, preferred_element_type=jnp.float32).astype(jnp.bfloat16),
        "tp",
        scatter_dimension=0,
        tiled=True,
    ).astype(jnp.float32)
    own_rows = lax.dynamic_slice_in_dim(residual, lax.axis_index("tp") * quarter, quarter, 0)
    rows_mid = (own_rows.astype(jnp.float32) + mixed).astype(jnp.bfloat16)
    own_normed = row_norm(rows_mid.astype(jnp.float32), mlp_gain).astype(jnp.bfloat16)
    normed = lax.all_gather(own_normed, "tp", axis=0, tiled=True)
    gate = jnp.dot(
        normed,
        lax.all_gather(gate_weight, "sp", axis=0, tiled=True),
        preferred_element_type=jnp.float32,
    )
    upvals = jnp.dot(
        normed,
        lax.all_gather(up_weight, "sp", axis=0, tiled=True),
        preferred_element_type=jnp.float32,
    )
    full_down = lax.all_gather(down_weight, "sp", axis=1, tiled=True)
    hidden = (jax.nn.silu(gate) * upvals).astype(jnp.bfloat16)
    picked = hidden
    ffn = lax.psum_scatter(
        jnp.dot(picked, full_down, preferred_element_type=jnp.float32).astype(jnp.bfloat16),
        "tp",
        scatter_dimension=0,
        tiled=True,
    ).astype(jnp.float32)
    return (rows_mid.astype(jnp.float32) + ffn).astype(jnp.bfloat16)


MESH = pl.DeviceIdType.MESH
XS = 2
CS = 2
F32 = jnp.float32
BF16 = jnp.bfloat16


def dot_nt(a, b):
    return lax.dot_general(a, b, (((1,), (1,)), ((), ())), preferred_element_type=F32)


def dot_nn(a, b):
    return lax.dot_general(a, b, (((1,), (0,)), ((), ())), preferred_element_type=F32)


def kernel(
    nz,
    nt,
    q_ref,
    k_ref,
    v_ref,
    g_ref,
    ld_ref,
    hg_ref,
    res_ref,
    mg_ref,
    ow_hbm,
    gw_hbm,
    uw_hbm,
    dw_hbm,
    out_ref,
    ow,
    raw,
    turned,
    w,
    qrot,
    inner,
    cumx,
    contrib,
    c_out,
    t_out,
    c_in,
    t_in,
    p_out,
    tt_out,
    p_in,
    tt_in,
    s_own,
    s_out,
    s_in,
    retained,
    mix_out,
    mix_in,
    acc,
    norm_own,
    normed,
    gated,
    hidden,
    keep,
    s1,
    r1,
    s2,
    r2,
    s3,
    r3,
    ow_sem,
    raw_sem,
    own_sem,
    w_send,
    w_recv,
    f_send,
    f_recv,
    cx_send,
    cx_recv,
    pz_send,
    pz_recv,
    sx_send,
    sx_recv,
    mix_send,
    mix_recv,
    nz_send,
    nz_recv,
    nt_send,
    nt_recv,
    t1_send,
    t1_recv,
    t2_send,
    t2_recv,
    t3_send,
    t3_recv,
):
    sp = lax.axis_index("sp")
    tp = lax.axis_index("tp")
    z, x = sp // XS, lax.rem(sp, XS)
    y, c = tp // CS, lax.rem(tp, CS)
    rows = q_ref.shape[0]
    heads = ld_ref.shape[0]
    hh = heads // XS
    hd = q_ref.shape[1] // heads
    quarter = rows // nt
    share, width = w.shape[2], w.shape[3]
    group = XS * width
    x_peer = (z * XS + (1 - x), tp)
    c_peer = (sp, y * CS + (1 - c))
    y_peer = (sp, (1 - y) * CS + c)

    def z_at(d):
        return lax.rem(z + d, nz)

    def z_from(d):
        return lax.rem(z - d + nz, nz)

    def z_peer(d):
        return (z_at(d) * XS + x, tp)

    def t_at(d):
        return lax.rem(tp + d, nt)

    def t_peer(d):
        return (sp, t_at(d))

    def remote(src, dst, send, recv, peer):
        return pltpu.make_async_remote_copy(
            src_ref=src,
            dst_ref=dst,
            send_sem=send,
            recv_sem=recv,
            device_id=peer,
            device_id_type=MESH,
        )

    started = []

    def go(copy):
        copy.start()
        started.append(copy)
        return copy

    def piece(m, zz):
        at = pl.ds(pl.multiple_of(zz * share, 16), share)
        return dw_hbm.at[at] if m == 2 else turned.at[m, at]

    raw_copies = []
    for m, source in enumerate((gw_hbm, uw_hbm)):
        raw_copy = pltpu.make_async_copy(source, raw.at[m], raw_sem.at[m])
        raw_copy.start()
        raw_copies.append(raw_copy)
    ow_copy = pltpu.make_async_copy(ow_hbm, ow, ow_sem)
    own_copies = {}

    def take_own(m):
        own_copies[m] = pltpu.make_async_copy(piece(m, z), w.at[m, sp], own_sem.at[m])
        own_copies[m].start()

    take_own(2)
    ow_copy.start()

    barrier = pltpu.get_barrier_semaphore()
    peers = [z_peer(d) for d in range(1, nz)] + [x_peer] + [t_peer(d) for d in range(1, nt)]
    for peer in peers:
        pl.semaphore_signal(barrier, inc=1, device_id=peer, device_id_type=MESH)
    for m in range(2):
        raw_copies[m].wait()
        for j in range(raw.shape[2] // 128):
            turned[m, j * 128 : (j + 1) * 128, :] = jnp.transpose(
                raw[m, :, j * 128 : (j + 1) * 128]
            )
        take_own(m)
    pl.semaphore_wait(barrier, len(peers))

    w_copies = {}

    def send_weight(m, d):
        w_copies[m, d] = go(
            remote(piece(m, z_at(d)), w.at[m, sp], w_send.at[m, d], w_recv.at[m, d], z_peer(d))
        )

    f_copies = {}

    def forward(m, d):
        slot = z_from(d) * XS + x
        if d == 0:
            own_copies[m].wait()
        else:
            w_copies[m, d].wait_recv()
        f_copies[m, d] = go(
            remote(w.at[m, slot], w.at[m, slot], f_send.at[m, d], f_recv.at[m, d], x_peer)
        )

    far = 2
    near = [d for d in range(1, nz) if d != far]
    send_weight(1, far)

    ti = lax.broadcasted_iota(jnp.int32, (rows, rows), 0)
    si = lax.broadcasted_iota(jnp.int32, (rows, rows), 1)
    lower = si <= ti
    cumul = lax.dot_general(
        ld_ref[...],
        (ti <= si).astype(F32),
        (((1,), (0,)), ((), ())),
        precision=lax.Precision.HIGHEST,
        preferred_element_type=F32,
    )
    half = hd // 2
    lane = lax.broadcasted_iota(jnp.int32, (1, hd), 1)
    low_half = lane < half
    index = jnp.where(low_half, lane, lane - half).astype(F32)
    freq = jnp.exp(index * (-math.log(10000.0) / (half - 1)))
    angles = (sp * rows + lax.broadcasted_iota(jnp.int32, (rows, hd), 0)).astype(F32) * freq
    cos = jnp.cos(angles)
    sin = jnp.sin(angles)
    sin = jnp.where(low_half, -sin, sin)
    for h in range(heads):
        cols = slice(h * hd, (h + 1) * hd)
        qf = q_ref[:, cols].astype(F32)
        kf = k_ref[:, cols].astype(F32)
        vb = v_ref[:, cols]
        qb = (qf * cos + pltpu.roll(qf, half, 1) * sin).astype(BF16)
        kb = ((kf * cos + pltpu.roll(kf, half, 1) * sin) * hd ** (-0.5)).astype(BF16)
        along = jnp.broadcast_to(cumul[h : h + 1, :], (rows, rows))
        cum = jnp.transpose(along)
        spread = cum - along
        weight = jnp.where(lower, jnp.exp(jnp.where(lower, spread, 0.0)), 0.0)
        probs = (dot_nt(qb, kb) * weight).astype(BF16)
        inner[:, cols] = dot_nn(probs, vb)
        last = cum[rows - 1 :, :]
        kw = kb.astype(F32) * jnp.exp(last - cum)
        cb = dot_nn(jnp.transpose(kw).astype(BF16), vb)
        contrib[h] = cb
        c_out[h] = cb.astype(BF16)
        t_out[h] = jnp.broadcast_to(jnp.exp(last), t_out.shape[1:])
        qrot[:, cols] = qb.astype(F32)
        cumx[:, cols] = jnp.exp(cum)
    mine_h, other_h = x * hh, (1 - x) * hh
    cx = go(remote(c_out.at[pl.ds(other_h, hh)], c_in, cx_send.at[0], cx_recv.at[0], x_peer))
    tx = go(remote(t_out, t_in, cx_send.at[1], cx_recv.at[1], x_peer))
    forward(1, 0)
    cx.wait_recv()
    tx.wait_recv()
    first = x == 0
    for i in range(hh):
        own_c, own_t = contrib[mine_h + i], t_out[mine_h + i][:1]
        other_c, other_t = c_in[i].astype(F32), t_in[mine_h + i][:1]
        plane = jnp.where(first, other_t * own_c + other_c, own_t * other_c + own_c)
        p_out[i] = plane.astype(BF16)
        tt_out[i] = jnp.broadcast_to(own_t * other_t, tt_out.shape[1:])
    pz, tz = {}, {}
    for d in range(1, nz):
        pz[d] = go(remote(p_out, p_in.at[z], pz_send.at[0, d], pz_recv.at[0, d], z_peer(d)))
        tz[d] = go(remote(tt_out, tt_in.at[z], pz_send.at[1, d], pz_recv.at[1, d], z_peer(d)))
    for d in range(1, nz):
        pz[d].wait_recv()
        tz[d].wait_recv()
    send_weight(0, far)
    send_weight(0, near[0])
    p_in[z] = p_out[...]
    tt_in[z] = tt_out[...]
    for i in range(hh):
        state = jnp.zeros((hd, hd), F32)
        for zz in range(nz - 1):
            later = tt_in[zz, i][:1] * state + p_in[zz, i].astype(F32)
            state = jnp.where(zz < z, later, state)
        early_t = jnp.where(first, t_out[mine_h + i][:1], t_in[mine_h + i][:1])
        early_c = jnp.where(first, contrib[mine_h + i], c_in[i].astype(F32))
        after = early_t * state + early_c
        s_own[i] = jnp.where(first, state, after)
        s_out[i] = jnp.where(first, after, state).astype(BF16)
    sx = go(remote(s_out, s_in, sx_send, sx_recv, x_peer))
    forward(0, 0)
    forward(1, far)

    def finish(h, state, cols):
        cross = lax.dot_general(
            qrot[:, cols],
            state,
            (((1,), (0,)), ((), ())),
            precision=lax.Precision.HIGHEST,
            preferred_element_type=F32,
        )
        ret = inner[:, cols] + cumx[:, cols] * cross
        scale = lax.rsqrt(jnp.mean(ret * ret, axis=-1, keepdims=True) + EPS)
        gf = g_ref[:, cols].astype(F32)
        retained[:, cols] = (
            ret * scale * hg_ref[:, cols] * (gf / (1.0 + jnp.exp(-gf)))
        ).astype(BF16)

    sx.wait_recv()
    for h in range(heads):
        cols = slice(h * hd, (h + 1) * hd)
        i = h % hh
        mine = x == h // hh
        finish(h, jnp.where(mine, s_own[i], s_in[i].astype(F32)), cols)
    ow_copy.wait()
    mixes = []
    for d in list(range(1, nt)) + [0]:
        mine = pl.multiple_of(t_at(d) * quarter, quarter)
        part = dot_nn(retained[pl.ds(mine, quarter), :], ow[...]).astype(BF16)
        if d == 0:
            mix_in[tp] = part
        else:
            mix_out[d] = part
            mixes.append(
                go(
                    remote(
                        mix_out.at[d], mix_in.at[tp], mix_send.at[d], mix_recv.at[d], t_peer(d)
                    )
                )
            )
    for mix in mixes:
        mix.wait_recv()
    mixed = mix_in[0].astype(F32)
    for j in range(1, nt):
        mixed += mix_in[j].astype(F32)
    mine = pl.multiple_of(tp * quarter, quarter)
    mid = (res_ref[pl.ds(mine, quarter), :].astype(F32) + mixed).astype(BF16).astype(F32)
    for g in range(nz):
        for u in range(XS):
            at = g * group + u * width
            acc[g, u] = mid[:, at : at + width]
    norm_own[...] = (
        mid * lax.rsqrt(jnp.mean(mid * mid, axis=-1, keepdims=True) + EPS) * mg_ref[...]
    ).astype(BF16)
    normed[z, tp] = norm_own[...]
    tcopy = {}

    def share_rows(i, zz):
        rows_at = normed.at[zz, tp]
        for e, peer in ((1, c_peer), (2, y_peer)):
            tcopy[i, e] = go(
                remote(rows_at, rows_at, nt_send.at[i, e], nt_recv.at[i, e], peer)
            )

    def pass_rows(i, zz):
        rows_at = normed.at[zz, (1 - y) * CS + c]
        tcopy[i, 2].wait_recv()
        tcopy[i, 3] = go(remote(rows_at, rows_at, nt_send.at[i, 3], nt_recv.at[i, 3], c_peer))

    mate = z + 1 - 2 * lax.rem(z, 2)
    mate_peer = (mate * XS + x, tp)
    z_far, z_last = z_from(far), lax.rem(mate + far, nz)
    n_far = go(remote(norm_own, normed.at[z, tp], nz_send.at[0], nz_recv.at[0], z_peer(far)))
    n_mate = go(remote(norm_own, normed.at[z, tp], nz_send.at[1], nz_recv.at[1], mate_peer))
    share_rows(0, z)
    forward(0, far)
    forward(2, 0)
    n_far.wait_recv()
    far_rows = normed.at[z_far, tp]
    n_pass = go(remote(far_rows, far_rows, nz_send.at[2], nz_recv.at[2], mate_peer))
    share_rows(1, z_far)
    send_weight(0, near[1])
    for d in near:
        send_weight(1, d)
    forward(0, near[0])
    n_mate.wait_recv()
    share_rows(2, mate)
    pass_rows(0, z)
    pass_rows(1, z_far)
    n_pass.wait_recv()
    share_rows(3, z_last)
    pass_rows(2, mate)
    forward(0, near[1])
    for d in [far] + near:
        send_weight(2, d)
    pass_rows(3, z_last)
    forward(1, near[0])
    for d in range(nz):
        f_copies[0, d].wait_recv()
    for key in sorted(tcopy):
        if key[1] != 2:
            tcopy[key].wait_recv()

    ns = nz * XS

    def project(m, zz):
        block = normed[zz].reshape(rows, normed.shape[3])
        total = dot_nt(block[:, :width], w[m, 0])
        for s in range(1, ns):
            total += dot_nt(block[:, s * width : (s + 1) * width], w[m, s])
        return total

    def gate_rows(zz):
        gate = project(0, zz)
        gated[zz] = gate / (1.0 + jnp.exp(-gate))

    def up_rows(zz):
        hidden[zz * rows : (zz + 1) * rows, :] = (gated[zz] * project(1, zz)).astype(BF16)

    for zz in range(nz // 2):
        gate_rows(zz)
    forward(1, near[1])
    for zz in range(nz // 2, nz):
        gate_rows(zz)
    forward(2, far)
    for d in range(nz):
        f_copies[1, d].wait_recv()
    for zz in range(nz):
        up_rows(zz)

    t1, t2, t3 = {}, {}, {}
    low = c == 0

    def side(u):
        return x if u == 0 else 1 - x

    def compute(b, u):
        if u:
            f_copies[2, b].wait_recv()
        part = dot_nn(hidden[...], w[2, z_from(b) * XS + side(u)])
        for zz in range(nz):
            for yy in range(nt // CS):
                at = zz * rows + yy * CS * quarter
                even = part[at : at + quarter]
                odd = part[at + quarter : at + 2 * quarter]
                keep[b, u, yy, zz] = jnp.where(low, even, odd)
                s1[b, u, yy, zz] = jnp.where(low, odd, even).astype(BF16)
        t1[b, u] = go(
            remote(s1.at[b, u], r1.at[b, u], t1_send.at[b, u], t1_recv.at[b, u], c_peer)
        )

    def second(b, u):
        t1[b, u].wait_recv()
        s2[b, u] = (keep[b, u, 1 - y] + r1[b, u, 1 - y].astype(F32)).astype(BF16)
        t2[b, u] = go(
            remote(s2.at[b, u], r2.at[b, u], t2_send.at[b, u], t2_recv.at[b, u], y_peer)
        )
        keep[b, u, y] = keep[b, u, y] + r1[b, u, y].astype(F32)

    def third(b, u):
        t2[b, u].wait_recv()
        for e in [far] + near:
            zz = z_at(e)
            s3[b, u, e] = (keep[b, u, y, zz] + r2[b, u, zz].astype(F32)).astype(BF16)
            t3[b, u, e] = go(
                remote(
                    s3.at[b, u, e],
                    r3.at[b, u, e],
                    t3_send.at[b, u, e],
                    t3_recv.at[b, u, e],
                    z_peer(e),
                )
            )
        g, v = z_from(b), side(u)
        acc[g, v] = acc[g, v] + keep[b, u, y, z] + r2[b, u, z].astype(F32)

    n0, n1 = near
    compute(0, 0)
    compute(0, 1)
    compute(far, 0)
    second(0, 0)
    second(0, 1)
    forward(2, n0)
    compute(n0, 0)
    compute(far, 1)
    second(far, 0)
    forward(2, n1)
    compute(n1, 0)
    second(n0, 0)
    second(far, 1)
    third(0, 0)
    third(0, 1)
    second(n1, 0)
    compute(n0, 1)
    third(far, 0)
    third(n0, 0)
    second(n0, 1)
    compute(n1, 1)
    third(far, 1)
    second(n1, 1)
    third(n1, 0)
    third(n0, 1)
    third(n1, 1)
    order = [(0, 0), (0, 1), (far, 0), (n0, 0), (far, 1), (n1, 0), (n0, 1), (n1, 1)]
    for b, u in order:
        for e in [far] + near:
            t3[b, u, e].wait_recv()
            g, v = lax.rem(z - e - b + 2 * nz, nz), side(u)
            acc[g, v] = acc[g, v] + r3[b, u, e].astype(F32)
    for g in range(nz):
        for u in range(XS):
            at = g * group + u * width
            out_ref[:, at : at + width] = acc[g, u].astype(BF16)
    for copy in started:
        copy.wait_send()


def fast_body(
    queries,
    key_rows,
    value_rows,
    gate_input,
    log_decay,
    head_gain,
    out_weight,
    residual,
    mlp_gain,
    gate_weight,
    up_weight,
    down_weight,
):
    rows, wide = queries.shape
    heads = log_decay.shape[1]
    hd = wide // heads
    model = residual.shape[1]
    ns, nt = lax.axis_size("sp"), lax.axis_size("tp")
    nz = ns // XS
    quarter = rows // nt
    width, units = gate_weight.shape
    share = units // nz
    group = XS * width
    hh = heads // XS
    vmem = pl.BlockSpec(memory_space=pltpu.VMEM)
    anyspace = pl.BlockSpec(memory_space=pl.ANY)
    dma = pltpu.SemaphoreType.DMA
    scratch = [
        pltpu.VMEM(out_weight.shape, BF16),
        pltpu.VMEM((2, width, units), BF16),
        pltpu.VMEM((2, units, width), BF16),
        pltpu.VMEM((3, ns, share, width), BF16),
        pltpu.VMEM((rows, wide), F32),
        pltpu.VMEM((rows, wide), F32),
        pltpu.VMEM((rows, wide), F32),
        pltpu.VMEM((heads, hd, hd), F32),
        pltpu.VMEM((heads, hd, hd), BF16),
        pltpu.VMEM((heads, 8, hd), F32),
        pltpu.VMEM((hh, hd, hd), BF16),
        pltpu.VMEM((heads, 8, hd), F32),
        pltpu.VMEM((hh, hd, hd), BF16),
        pltpu.VMEM((hh, 8, hd), F32),
        pltpu.VMEM((nz, hh, hd, hd), BF16),
        pltpu.VMEM((nz, hh, 8, hd), F32),
        pltpu.VMEM((hh, hd, hd), F32),
        pltpu.VMEM((hh, hd, hd), BF16),
        pltpu.VMEM((hh, hd, hd), BF16),
        pltpu.VMEM((rows, wide), BF16),
        pltpu.VMEM((nt, quarter, model), BF16),
        pltpu.VMEM((nt, quarter, model), BF16),
        pltpu.VMEM((nz, XS, quarter, width), F32),
        pltpu.VMEM((quarter, model), BF16),
        pltpu.VMEM((nz, nt, quarter, model), BF16),
        pltpu.VMEM((nz, rows, share), F32),
        pltpu.VMEM((nz * rows, share), BF16),
        pltpu.VMEM((nz, XS, nt // CS, nz, quarter, width), F32),
        pltpu.VMEM((nz, XS, nt // CS, nz, quarter, width), BF16),
        pltpu.VMEM((nz, XS, nt // CS, nz, quarter, width), BF16),
        pltpu.VMEM((nz, XS, nz, quarter, width), BF16),
        pltpu.VMEM((nz, XS, nz, quarter, width), BF16),
        pltpu.VMEM((nz, XS, nz, quarter, width), BF16),
        pltpu.VMEM((nz, XS, nz, quarter, width), BF16),
        dma,
        dma((2,)),
        dma((3,)),
        dma((3, nz)),
        dma((3, nz)),
        dma((3, nz)),
        dma((3, nz)),
        dma((2,)),
        dma((2,)),
        dma((2, nz)),
        dma((2, nz)),
        dma,
        dma,
        dma((nt,)),
        dma((nt,)),
        dma((nz,)),
        dma((nz,)),
        dma((nz, nt)),
        dma((nz, nt)),
        dma((nz, XS)),
        dma((nz, XS)),
        dma((nz, XS)),
        dma((nz, XS)),
        dma((nz, XS, nz)),
        dma((nz, XS, nz)),
    ]
    return pl.pallas_call(
        functools.partial(kernel, nz, nt),
        out_shape=jax.ShapeDtypeStruct((quarter, model), BF16),
        in_specs=[vmem] * 8 + [anyspace] * 4,
        out_specs=vmem,
        scratch_shapes=scratch,
        compiler_params=pltpu.CompilerParams(
            collective_id=0, has_side_effects=True, vmem_limit_bytes=60 * 1024 * 1024
        ),
    )(
        queries,
        key_rows,
        value_rows,
        gate_input,
        log_decay.T,
        head_gain.reshape(1, wide),
        residual,
        mlp_gain.reshape(1, model),
        out_weight,
        gate_weight,
        up_weight,
        down_weight,
    )


def fits(mesh, queries, log_decay, gate_weight):
    ns, nt = mesh.shape["sp"], mesh.shape["tp"]
    tokens, wide = queries.shape
    if ns % XS or ns // XS != 4 or nt != 2 * CS or tokens // ns != BLOCK:
        return False
    nz = ns // XS
    hidden = gate_weight.shape[1] // nt
    return (
        gate_weight.shape[0] // ns % 128 == 0
        and hidden % (16 * nz) == 0
        and wide // log_decay.shape[1] == 128
        and BLOCK % (16 * nt) == 0
        and hidden % 128 == 0
        and log_decay.shape[1] // nt % XS == 0
    )


def solution(mesh):
    def run(*args):
        good = fits(mesh, args[0], args[4], args[9])
        return jax.shard_map(
            fast_body if good else body,
            mesh=mesh,
            in_specs=(
                P("sp", "tp"),
                P("sp", "tp"),
                P("sp", "tp"),
                P("sp", "tp"),
                P("sp", "tp"),
                P("tp"),
                P("tp", None),
                P("sp", None),
                P(),
                P("sp", "tp"),
                P("sp", "tp"),
                P("tp", "sp"),
            ),
            out_specs=P(("sp", "tp"), None),
            check_vma=False,
        )(*args)

    return run
```
